32 devices in a mesh: sp: 8 (over z, y), tp: 4 (over x, core).
Axes of the slice: x: 2, y: 2, z: 4, core: 2. Of those that a mesh axis runs over, the one named last changes fastest.
Arguments:
- tokens: bfloat16 [4096, 2048], P(('sp', 'tp')), may hold values from -6 to 6
- queries: bfloat16 [4096, 1024], P('sp', 'tp'), may hold values from -160 to 160
- keys: bfloat16 [4096, 1024], P('sp', 'tp'), may hold values from -8 to 8
- values: bfloat16 [4096, 1024], P('sp', 'tp'), may hold values from -6 to 6
- lambdas: float32 [8], P('tp'), may hold values from 0.3 to 0.8
- head_gain: float32 [128], replicated, may hold values from 0.1 to 1.9
- out_weight: bfloat16 [1024, 2048], replicated, may hold values from -0.1875 to 0.1875
- mixer_gain: float32 [2048], replicated, may hold values from 0.1 to 1.9
- up_weight: bfloat16 [2048, 4096], P('sp', 'tp'), may hold values from -0.125 to 0.125
- down_weight: bfloat16 [4096, 2048], P('tp', 'sp'), may hold values from -0.09375 to 0.09375
Outputs:
- result: bfloat16 [4096, 2048], P(('sp', 'tp'))
The draws below stay inside these ranges and needn't reach their ends.
All inputs are finite; a program needn't handle non-finite values.
Results may differ from the reference program's by a relative error of at most 0.02.
Values may be sent and summed in bfloat16 or wider, within the bound.
A program may use at most 128 MiB of HBM per device.

```python
import math
import jax
import jax.numpy as jnp
from jax import lax

D = 2048
HEADS = 8
DQK = 64
DV = 128
ATTN = 1024
FF = 4096
TOKENS = 4096


def drawn(key):
    base = jax.random.normal(jax.random.fold_in(key, 11), (TOKENS, HEADS * 2 * DQK), jnp.float32) * 1.3
    base = jnp.clip(base, -7.8, 7.8)
    return base


def draw_keys(key, part):
    base = drawn(key)
    return base.astype(jnp.bfloat16)


def draw_queries(key, part):
    own = jax.random.normal(jax.random.fold_in(key, 21), (TOKENS, HEADS * 2 * DQK), jnp.float32) * 1.3
    own = jnp.clip(own, -7.8, 7.8)
    return own.astype(jnp.bfloat16)


def steps_of(own_key, shape, pieces, least, top_value):
    loudness = 1.0
    for position, blocks in pieces:
        steps = jax.random.uniform(jax.random.fold_in(jax.random.fold_in(own_key, 6), position), (blocks,), jnp.float32, least / len(pieces), top_value / len(pieces))
        loudness = loudness * jnp.repeat(jnp.exp(steps), shape[position] // blocks).reshape((-1,) + (1,) * (len(shape) - 1 - position))
    return loudness


def bell_draw(key, dims, width, most, cuts=(), kind=jnp.bfloat16):
    entries = jax.random.normal(key, dims, jnp.float32) * width
    if len(cuts) > 0:
        entries = steps_of(key, dims, cuts, -0.22, 0.18) * entries
    return jnp.clip(entries, min=-most, max=most).astype(kind)


def setup_inputs(seed: int = 0) -> dict:
    splits = jax.random.split(jax.random.key(seed), 11)
    tokens = bell_draw(splits[0], (TOKENS, D), 1.0, 6.0, ((0, 32),))
    queries = draw_queries(jax.random.fold_in(splits[10], 71), 0)
    keys = draw_keys(jax.random.fold_in(splits[10], 71), 0)
    values = bell_draw(splits[3], (TOKENS, ATTN), 1.0, 6.0, ((0, 8), (1, 4)))
    lambdas = jnp.clip(0.3 + 0.5 * jax.random.uniform(splits[4], (HEADS,), jnp.float32) ** steps_of(splits[4], (HEADS,), ((0, 4),), -0.2, 0.2), 0.3, 0.8)
    head_gain = jnp.clip(1.0 + 0.18 * jax.random.normal(splits[5], (DV,), jnp.float32), 0.1, 1.9)
    out_weight = bell_draw(splits[6], (ATTN, D), ATTN ** -0.5, 0.1875)
    mixer_gain = jnp.clip(1.0 + 0.18 * jax.random.normal(splits[7], (D,), jnp.float32), 0.1, 1.9)
    up_weight = bell_draw(splits[8], (D, FF), D ** -0.5, 0.125, ((0, 8), (1, 4)))
    down_weight = bell_draw(splits[9], (FF, D), FF ** -0.5, 0.09375, ((0, 4), (1, 8)))
    return {"tokens": tokens, "queries": queries, "keys": keys, "values": values, "lambdas": lambdas, "head_gain": head_gain, "out_weight": out_weight, "mixer_gain": mixer_gain, "up_weight": up_weight, "down_weight": down_weight}


def reference(tokens, queries, keys, values, lambdas, head_gain, out_weight, mixer_gain, up_weight, down_weight):
    query_heads = jnp.transpose(queries.astype(jnp.float32).reshape(TOKENS, HEADS, 2, DQK), (1, 2, 0, 3))
    key_heads = jnp.transpose(keys.astype(jnp.float32).reshape(TOKENS, HEADS, 2, DQK), (1, 2, 0, 3))
    value_heads = jnp.transpose(values.astype(jnp.float32).reshape(TOKENS, HEADS, DV), (1, 0, 2))
    block_rows = math.gcd(TOKENS, 512)
    positions = jnp.arange(TOKENS, dtype=jnp.int32)

    def one_head(inputs):
        query_pair, key_pair, value_rows, lam_value = inputs

        def one_block(block_index):
            offset = (block_index * block_rows).astype(jnp.int32)
            query_pos = offset + jnp.arange(block_rows, dtype=jnp.int32)
            allowed = positions[None, :] <= query_pos[:, None]
            head_maps = []
            for map_index in range(2):
                query_rows = lax.dynamic_slice_in_dim(query_pair[map_index], offset, block_rows, 0)
                scores = jnp.dot(query_rows, key_pair[map_index].T, precision=lax.Precision.HIGHEST, preferred_element_type=jnp.float32) * DQK ** (-0.5)
                scores = jnp.where(allowed, scores, -jnp.inf)
                row_max = lax.optimization_barrier(jnp.max(scores, axis=1, keepdims=True))
                exponent = jnp.exp(scores - row_max)
                row_total = lax.optimization_barrier(jnp.sum(exponent, axis=1, keepdims=True))
                weights = lax.optimization_barrier(exponent.astype(jnp.bfloat16)).astype(jnp.float32)
                head_maps.append(jnp.dot(weights, value_rows, precision=lax.Precision.HIGHEST, preferred_element_type=jnp.float32) / row_total)
            differ = head_maps[0] - lam_value * head_maps[1]
            spread = lax.rsqrt(lax.optimization_barrier(jnp.mean(differ * differ, axis=1, keepdims=True)) + 1e-06)
            return (differ * spread * head_gain).astype(jnp.bfloat16)
        return lax.map(one_block, jnp.arange(TOKENS // block_rows, dtype=jnp.int32))
    attended = lax.map(one_head, (query_heads, key_heads, value_heads, lambdas))
    attended = jnp.transpose(attended.reshape(HEADS, TOKENS, DV), (1, 0, 2)).reshape(TOKENS, HEADS * DV)
    projected = jnp.dot(attended, out_weight, preferred_element_type=jnp.float32).astype(jnp.bfloat16)
    resid = (tokens.astype(jnp.float32) + projected.astype(jnp.float32)).astype(jnp.bfloat16)
    resid_full = resid.astype(jnp.float32)
    normed = (resid_full * lax.rsqrt(lax.optimization_barrier(jnp.mean(resid_full * resid_full, axis=1, keepdims=True)) + 1e-06) * mixer_gain).astype(jnp.bfloat16)
    hidden = jnp.square(jax.nn.relu(jnp.dot(normed, up_weight, preferred_element_type=jnp.float32))).astype(jnp.bfloat16)
    return (resid_full + jnp.dot(hidden, down_weight, preferred_element_type=jnp.float32)).astype(jnp.bfloat16)
```

```python
import functools

import jax
import jax.numpy as jnp
from jax import lax
from jax.experimental import pallas as pl
from jax.experimental.pallas import tpu as pltpu
from jax.sharding import PartitionSpec as P

DQK = 64
MESH = pl.DeviceIdType.MESH
f32, bf16 = jnp.float32, jnp.bfloat16
CHUNKS = 4
UPS, DOWNS = (0, 1), (2, 3)


def layer_kernel(
    n, tp,
    lam_ref, q_ref, k_ref, v_ref, gain_ref, up_ref, dn_ref, tok_ref, mix_ref, ow_hbm,
    out_ref,
    ah, upf_ref, dnf_ref,
    qb, kv, qm, run_max, run_sum, acc, att, att_above, ow, tokall, normed, hsum, hid, part, core_in, cross, cross_in,
    ex_send, ex_recv, top_recv, swap_send, tk_send, tk_recv, kv_send, kv_recv,
    w_send, own_send, y_send, w_recv, u_send, u_recv, a_send, a_recv, loc,
    c_send, c_recv, x_send, x_recv,
):
    s = lax.axis_index("sp")
    t = lax.axis_index("tp")
    z, y = s // 2, lax.rem(s, 2)
    x, c = t // 2, lax.rem(t, 2)
    steps = n // 2
    rows = q_ref.shape[0]
    wide = q_ref.shape[1] // 2
    total = 2 * rows
    piece = rows // tp
    top, helper = z == steps - 1, z == steps - 2
    has_up, has_down = z < steps - 1, z > 0
    above, below = (s + 2, t), (s - 2, t)
    beside = (s + 1 - 2 * y, t)
    core = (s, t + 1 - 2 * c)
    across_x = (s, lax.rem(t + 2, tp))
    corner = (s + 1 - 2 * y, lax.rem(t + 2, tp))
    line = 2 * z + c
    own_line = y == c
    partner = (line, 2 * x + y)

    barrier = pltpu.get_barrier_semaphore()

    def greet(device):
        pl.semaphore_signal(barrier, inc=1, device_id=device, device_id_type=MESH)

    for e in range(2):
        for i in range(tp):
            who = (2 * z + e, i)

            @pl.when(jnp.logical_or(e != y, i != t))
            def _():
                greet(who)

    pl.when(has_up)(lambda: greet(above))
    pl.when(has_down)(lambda: greet(below))
    pl.when(top)(lambda: greet((s - 2 + 1 - 2 * y, t)))
    pl.when(helper)(lambda: greet((s + 2 + 1 - 2 * y, t)))
    pl.semaphore_wait(
        barrier,
        2 * tp - 1 + has_up.astype(jnp.int32) + has_down.astype(jnp.int32)
        + jnp.logical_or(top, helper).astype(jnp.int32),
    )

    def remote(src, dst, send, recv, device):
        return pltpu.make_async_remote_copy(
            src_ref=src, dst_ref=dst, send_sem=send, recv_sem=recv, device_id=device, device_id_type=MESH
        )

    def rows_of(e):
        return pl.ds(pl.multiple_of(e * rows, rows), rows)

    def cols_of(e):
        return pl.ds(pl.multiple_of(e * wide, wide), wide)

    my_rows, peer_rows = rows_of(y), rows_of(1 - y)
    my_cols, peer_cols = cols_of(y), cols_of(1 - y)
    qkv = (q_ref, k_ref, v_ref)

    def landing(i, plane, slot, where):
        return qb.at[slot, where] if i == 0 else kv.at[plane, i - 1, where]

    def exchange(i, where):
        return remote(
            qkv[i].at[:, peer_cols], landing(i, z, 0, where), ex_send.at[0, i], ex_recv.at[i], beside
        )

    def lower(i, e):
        cols = my_cols if e == 0 else peer_cols
        device = below if e == 0 else (s - 2 + 1 - 2 * y, t)
        return remote(
            qkv[i].at[:, cols], landing(i, z, 1, my_rows), ex_send.at[e, i], top_recv.at[y, i], device
        )

    @pl.when(jnp.logical_not(top))
    def _():
        for i in (1, 2, 0):
            exchange(i, my_rows).start()

    @pl.when(top)
    def _():
        for i in range(3):
            for e in range(2):
                lower(i, e).start()

    depth, units = up_ref.shape
    half_depth, half = depth // 2, units // 2

    def shard(k, j):
        if k in UPS:
            return upf_ref.at[pl.ds(pl.multiple_of(j * depth + k * half_depth, half_depth), half_depth)]
        return dnf_ref.at[j, slice((k - 2) * half, (k - 1) * half)]

    given = (
        up_ref.at[slice(0, half_depth)], up_ref.at[slice(half_depth, depth)],
        dn_ref.at[slice(0, half)], dn_ref.at[slice(half, units)],
    )

    def swap(k):
        return remote(given[k], shard(k, s), swap_send.at[k], w_recv.at[s, k], partner)

    def send_above(k, j, src):
        remote(src, shard(k, j), w_send.at[j, k], w_recv.at[j, k], above).start()

    def send_below(k, j, src, sems):
        remote(src, shard(k, j), sems, w_recv.at[j, k], below).start()

    def over(k, j, src):
        remote(src, shard(k, j), y_send.at[j, k], w_recv.at[j, k], core).start()

    early_down = jnp.logical_or(z == 0, helper)

    def own_above(k, src):
        pl.when(has_up)(lambda: send_above(k, line, src))

    def own_around(k, src):
        pl.when(has_down)(lambda: send_below(k, line, src, own_send.at[k]))
        over(k, line, src)

    @pl.when(own_line)
    def _():
        for k in UPS:
            own_above(k, given[k])
        for k in UPS + DOWNS:
            own_around(k, given[k])

    @pl.when(jnp.logical_not(own_line))
    def _():
        for k in UPS + DOWNS:
            swap(k).start()

    def band(i):
        return pl.ds(pl.multiple_of(i * piece, piece), piece)

    b = 2 * y + x
    bx = b + 1 - 2 * x
    by = lax.rem(b + 2, tp)
    bd = lax.rem(bx + 2, tp)

    def token_copy(k, source, device):
        return remote(tok_ref, tokall.at[band(source)], tk_send.at[k], tk_recv.at[source], device)

    token_copy(0, b, across_x).start()

    def local_copy(i):
        src, dst = (
            (k_ref.at[:, my_cols], kv.at[z, 0, my_rows]),
            (v_ref.at[:, my_cols], kv.at[z, 1, my_rows]),
            (q_ref.at[:, my_cols], qb.at[0, my_rows]),
            (up_ref, upf_ref.at[pl.ds(pl.multiple_of(s * depth, depth), depth)]),
            (dn_ref, dnf_ref.at[s]),
            (ow_hbm, ow),
            (tok_ref, tokall.at[band(b)]),
        )[i]
        return pltpu.make_async_copy(src, dst, loc.at[i])

    @pl.when(jnp.logical_not(top))
    def _():
        for i in range(3):
            local_copy(i).start()

    @pl.when(own_line)
    def _():
        local_copy(3).start()
        local_copy(4).start()

    local_copy(5).start()
    local_copy(6).start()

    def kv_up(j):
        return remote(kv.at[j], kv.at[j], kv_send.at[j], kv_recv.at[j], above)

    kv_rises = z < steps - 2

    @pl.when(jnp.logical_not(top))
    def _():
        for i in range(3):
            local_copy(i).wait()
        for i in (1, 2, 0):
            exchange(i, peer_rows).wait_recv()
        pl.when(kv_rises)(lambda: kv_up(z).start())

    @pl.when(jnp.logical_and(own_line, early_down))
    def _():
        for k in DOWNS:
            own_above(k, given[k])

    def await_chunk(k, j):
        moved = shard(k, j)
        remote(moved, moved, w_send.at[j, k], w_recv.at[j, k], core).wait_recv()

    def swapped(ks):
        @pl.when(jnp.logical_not(own_line))
        def _():
            for k in ks:
                await_chunk(k, line)
                src = shard(k, line)
                if k in UPS:
                    own_above(k, src)
                else:
                    pl.when(early_down)(lambda: own_above(k, src))
                own_around(k, src)

    def late_down():
        @pl.when(own_line)
        def _():
            for k in DOWNS:
                own_above(k, given[k])

        @pl.when(jnp.logical_not(own_line))
        def _():
            for k in DOWNS:
                own_above(k, shard(k, line))

    def from_above(d, ks):
        j = line + 2 * d
        for k in ks:
            await_chunk(k, j)
            src = shard(k, j)
            pl.when(has_down)(lambda: send_below(k, j, src, w_send.at[j, k]))
            over(k, j, src)

    def from_below(d, ks):
        j = line - 2 * d
        for k in ks:
            await_chunk(k, j)
            src = shard(k, j)
            pl.when(has_up)(lambda: send_above(k, j, src))
            over(k, j, src)

    chunk = min(512, total)
    lane = lax.broadcasted_iota(jnp.int32, (total, wide), 1)

    def weigh(sc, top_row):
        parts, whole = [], None
        for i in range(sc.shape[1] // 128):
            p = jnp.exp(sc[:, i * 128:(i + 1) * 128] - top_row)
            whole = p if whole is None else whole + p
            parts.append(p.astype(bf16))
        return jnp.concatenate(parts, axis=1), whole

    def scores_of(u, r0, j, keys):
        return lax.dot_general(
            qm[u, pl.ds(r0, chunk), :], kv[j, 0, :keys, :], (((1,), (1,)), ((), ())), preferred_element_type=f32
        )

    def diagonal(u, carry):
        @pl.when(u == 1)
        def _():
            for e in range(2):
                for i in range(3):
                    dst = landing(i, z + 1, 1, rows_of(e))
                    remote(dst, dst, ex_send.at[0, i], top_recv.at[e, i], above).wait_recv()

        scaled = qb[u] * jnp.asarray(DQK ** -0.5, bf16)
        for m in range(2):
            qm[u, m * total:(m + 1) * total, :] = jnp.where((lane < DQK) == (m == 0), scaled, jnp.zeros_like(scaled))
        j = z + u
        for m in range(2):
            for i in range(total // chunk):
                r0, keys = m * total + i * chunk, (i + 1) * chunk
                here = pl.ds(r0, chunk)
                sc = scores_of(u, r0, j, keys)
                qpos = i * chunk + lax.broadcasted_iota(jnp.int32, (chunk, keys), 0)
                kpos = lax.broadcasted_iota(jnp.int32, (chunk, keys), 1)
                sc = jnp.where(kpos <= qpos, sc, -jnp.inf)
                top_row = jnp.broadcast_to(jnp.max(sc, axis=1, keepdims=True), (chunk, 128))
                p, whole = weigh(sc, top_row)
                run_max[u, here, :] = top_row
                run_sum[u, here, :] = whole
                acc[u, here, :] = jnp.dot(p, kv[j, 1, :keys, :], preferred_element_type=f32)
        return carry

    def tiles(u, j):
        def tile(i, carry):
            r0 = pl.multiple_of(i * chunk, chunk)
            here = pl.ds(r0, chunk)
            sc = scores_of(u, r0, j, total)
            old = run_max[u, here, :]
            top_row = jnp.maximum(old, jnp.max(sc, axis=1, keepdims=True))
            p, whole = weigh(sc, top_row)
            shrink = jnp.exp(old - top_row)
            run_max[u, here, :] = top_row
            run_sum[u, here, :] = run_sum[u, here, :] * shrink + whole
            acc[u, here, :] = acc[u, here, :] * shrink + jnp.dot(p, kv[j, 1], preferred_element_type=f32)
            return carry

        lax.fori_loop(0, 2 * total // chunk, tile, 0)

    def finish(u, dst):
        lam = lam_ref[y]
        maps = []
        for m in range(2):
            here = slice(m * total, (m + 1) * total)
            maps.append(acc[u, here, :] / jnp.sum(run_sum[u, here, :], axis=1, keepdims=True))
        differ = maps[0] - lam * maps[1]
        spread = lax.rsqrt(jnp.mean(differ * differ, axis=1, keepdims=True) + 1e-06)
        dst[...] = (differ * spread * gain_ref[...]).astype(bf16).reshape(dst.shape)

    def raise_att():
        return remote(att_above, att, u_send.at[0], u_recv.at[0], above)

    @pl.when(jnp.logical_not(top))
    def _():
        diagonal(0, 0)

    swapped(UPS)

    @pl.when(helper)
    def _():
        lax.fori_loop(1, 2, diagonal, 0)
        tiles(1, z)

    swapped(DOWNS)
    token_copy(1, b, beside).start()
    token_copy(2, b, corner).start()

    def block(d, carry):
        j = z - d
        kv_up(j).wait_recv()
        pl.when(kv_rises)(lambda: kv_up(j).start())

        def slot(v, inner):
            u = 1 - v

            @pl.when(jnp.logical_and(u == 0, d == 2))
            def _():
                from_below(1, UPS)

            tiles(u, j)

            @pl.when(jnp.logical_and(u == 1, d == z))
            def _():
                finish(1, att_above)
                raise_att().start()

            return inner

        lax.fori_loop(jnp.where(helper, 0, 1), 2, slot, 0)
        pl.when(d == 1)(lambda: from_above(1, UPS))
        pl.when(d == 2)(lambda: from_above(1, DOWNS))
        return carry

    lax.fori_loop(1, jnp.where(top, 1, z + 1), block, 0)
    pl.when(jnp.logical_not(top))(lambda: finish(0, att))

    @pl.when(top)
    def _():
        from_below(1, UPS + DOWNS)
        from_below(2, UPS)
        raise_att().wait_recv()

    head = 2 * t + y

    def head_cols(i):
        return pl.ds(pl.multiple_of(i * wide, wide), wide)

    def to_tokens(e, i, owner):
        return remote(
            att.at[:, i % 2], ah.at[:, :, head_cols(owner)], a_send.at[e * tp + i], a_recv.at[owner], (2 * z + e, i)
        )

    mine = pltpu.make_async_copy(att.at[:, c], ah.at[:, :, head_cols(head)], loc.at[7])
    mine.start()
    for e in range(2):
        for i in range(tp):
            pl.when(jnp.logical_or(e != y, i != t))(lambda: to_tokens(e, i, head).start())

    @pl.when(z == 0)
    def _():
        from_above(1, UPS + DOWNS)

    @pl.when(z == 1)
    def _():
        from_above(1, DOWNS)
        from_below(1, UPS)
        late_down()

    @pl.when(jnp.logical_and(z >= 2, has_up))
    def _():
        from_below(2, UPS)

    @pl.when(top)
    def _():
        from_below(3, UPS)

    local_copy(5).wait()
    local_copy(6).wait()
    mine.wait()
    for k, (source, device) in enumerate(((bx, across_x), (by, beside), (bd, corner))):
        token_copy(k, source, device).wait_recv()
    for i in range(2 * tp):
        e, who = i % 2, i // 2
        pl.when(jnp.logical_or(e != y, who != t))(lambda: to_tokens(0, 0, i).wait_recv())

    def project(i, carry):
        span = pl.ds(pl.multiple_of(2 * i * piece, 2 * piece), 2 * piece)
        heads = ah[pl.ds(2 * i, 2)].reshape(2 * piece, 2 * tp * wide)
        projected = jnp.dot(heads, ow[...], preferred_element_type=f32).astype(bf16)
        summed = (tokall[span, :].astype(f32) + projected.astype(f32)).astype(bf16)
        tokall[span, :] = summed
        summed = summed.astype(f32)
        scale = lax.rsqrt(jnp.mean(summed * summed, axis=1, keepdims=True) + 1e-06)
        normed[span, :] = (summed * scale * mix_ref[...]).astype(bf16)
        return carry

    lax.fori_loop(0, tp // 2, project, 0)

    def later_ups(d, carry):
        pl.when(z + d < steps)(lambda: from_above(d, UPS))
        waits = jnp.logical_and(d >= 3, jnp.logical_not(jnp.logical_and(top, d == 3)))
        pl.when(jnp.logical_and(z - d >= 0, waits))(lambda: from_below(d, UPS))
        return carry

    lax.fori_loop(2, steps, later_ups, 0)
    pl.when(jnp.logical_and(z > 1, kv_rises))(late_down)
    pl.when(jnp.logical_and(z >= 1, has_up))(lambda: from_below(1, DOWNS))

    @pl.when(own_line)
    def _():
        local_copy(3).wait()
        local_copy(4).wait()

    def order(k):
        return jnp.where(k < steps - z, z + k, steps - 1 - k)

    def from_core(k, i):
        await_chunk(k, 2 * i + 1 - c)

    pair_depth = 2 * depth
    hsum[...] = jnp.zeros_like(hsum)

    def up_pair(k, carry):
        i = order(k)
        for m in UPS:
            from_core(m, i)
        span = pl.ds(pl.multiple_of(i * pair_depth, pair_depth), pair_depth)
        hsum[...] += jnp.dot(normed[:, span], upf_ref[span, :], preferred_element_type=f32)
        return carry

    lax.fori_loop(0, steps, up_pair, 0)
    hid[...] = jnp.square(jnp.maximum(hsum[...], 0.0)).astype(bf16)

    first = ((across_x, bx), (beside, by))

    def to_first(j, e, m):
        device, where = first[e]
        return remote(
            part.at[j, band(where if m == 0 else bd)], core_in.at[j, m], c_send.at[j, m], c_recv.at[j, m], device
        )

    def to_second(j, e):
        return remote(cross.at[j], cross_in.at[j], x_send.at[j], x_recv.at[j], first[1 - e][0])

    def relay(i):
        for e in range(2):
            j = 2 * i + e
            to_first(j, e, 1).wait_recv()
            where = first[1 - e][1]
            cross[j] = (part[j, band(where), :].astype(f32) + core_in[j, 1].astype(f32)).astype(bf16)
            to_second(j, e).start()

    def down_pair(k, carry):
        i = order(k)
        last = k == steps - 1
        pl.when(last)(lambda: relay(order(k - 1)))
        pl.when(i - z >= 2)(lambda: from_above(i - z, DOWNS))
        pl.when(z - i >= 2)(lambda: from_below(z - i, DOWNS))
        for m in DOWNS:
            from_core(m, i)
        for e in range(2):
            j = 2 * i + e
            part[j] = jnp.dot(hid[...], dnf_ref[j], preferred_element_type=f32).astype(bf16)
            to_first(j, e, 1).start()
            to_first(j, e, 0).start()
        pl.when(jnp.logical_and(k > 0, k < steps - 1))(lambda: relay(order(k - 1)))
        return carry

    lax.fori_loop(0, steps, down_pair, 0)
    relay(order(steps - 1))

    cols = dn_ref.shape[1]
    for j in reversed(range(n)):
        to_first(j, j % 2, 0).wait_recv()
        to_second(j, j % 2).wait_recv()
        here = slice(j * cols, (j + 1) * cols)
        both = part[j, band(b), :].astype(f32) + core_in[j, 0].astype(f32) + cross_in[j].astype(f32)
        out_ref[:, here] = (tokall[band(b), here].astype(f32) + both).astype(bf16)

    for j in range(n):
        to_first(j, j % 2, 0).wait_send()
        to_first(j, j % 2, 1).wait_send()
        to_second(j, j % 2).wait_send()
    for k, device in enumerate((across_x, beside, corner)):
        token_copy(k, b, device).wait_send()
    for e in range(2):
        for i in range(tp):
            pl.when(jnp.logical_or(e != y, i != t))(lambda: to_tokens(e, i, head).wait_send())

    @pl.when(jnp.logical_not(top))
    def _():
        for i in range(3):
            exchange(i, my_rows).wait_send()

    @pl.when(top)
    def _():
        for i in range(3):
            for e in range(2):
                lower(i, e).wait_send()

    @pl.when(jnp.logical_not(own_line))
    def _():
        for k in UPS + DOWNS:
            swap(k).wait_send()

    pl.when(helper)(lambda: raise_att().wait_send())

    @pl.when(kv_rises)
    def _():
        def sent(j, carry):
            kv_up(j).wait_send()
            return carry

        lax.fori_loop(0, z + 1, sent, 0)

    def line_sent(i, carry):
        j = 2 * i + c
        for k in UPS + DOWNS:
            moved = shard(k, j)
            remote(moved, moved, y_send.at[j, k], w_recv.at[j, k], core).wait_send()
            gone = jnp.logical_or(jnp.logical_and(i <= z, has_up), jnp.logical_and(i > z, has_down))
            pl.when(gone)(lambda: remote(moved, moved, w_send.at[j, k], w_recv.at[j, k], core).wait_send())
        return carry

    lax.fori_loop(0, steps, line_sent, 0)

    @pl.when(has_down)
    def _():
        for k in UPS + DOWNS:
            moved = shard(k, line)
            remote(moved, moved, own_send.at[k], w_recv.at[line, k], core).wait_send()


def per_device(
    n, tp, tokens, queries, keys, values, lambdas, head_gain, out_weight, mixer_gain, up_weight, down_weight
):
    rows, wide = queries.shape[0], queries.shape[1] // 2
    depth, units = up_weight.shape
    cols = down_weight.shape[1]
    piece, width = tokens.shape
    total = 2 * rows
    vmem = pl.BlockSpec(memory_space=pltpu.VMEM)
    dma = pltpu.SemaphoreType.DMA
    return pl.pallas_call(
        functools.partial(layer_kernel, n, tp),
        out_shape=jax.ShapeDtypeStruct(tokens.shape, bf16),
        in_specs=[pl.BlockSpec(memory_space=pltpu.SMEM)] + [vmem] * 8 + [pl.BlockSpec(memory_space=pl.ANY)],
        out_specs=vmem,
        scratch_shapes=[
            pltpu.VMEM((tp, piece, 2 * tp * wide), bf16),
            pltpu.VMEM((n * depth, units), bf16),
            pltpu.VMEM((n, units, cols), bf16),
            pltpu.VMEM((2, total, wide), bf16),
            pltpu.VMEM((n // 2, 2, total, wide), bf16),
            pltpu.VMEM((2, 2 * total, wide), bf16),
            pltpu.VMEM((2, 2 * total, 128), f32),
            pltpu.VMEM((2, 2 * total, 128), f32),
            pltpu.VMEM((2, 2 * total, wide), f32),
            pltpu.VMEM((tp, 2, piece, wide), bf16),
            pltpu.VMEM((tp, 2, piece, wide), bf16),
            pltpu.VMEM(out_weight.shape, bf16),
            pltpu.VMEM((rows, width), bf16),
            pltpu.VMEM((rows, width), bf16),
            pltpu.VMEM((rows, units), f32),
            pltpu.VMEM((rows, units), bf16),
            pltpu.VMEM((n, rows, cols), bf16),
            pltpu.VMEM((n, 2, piece, cols), bf16),
            pltpu.VMEM((n, piece, cols), bf16),
            pltpu.VMEM((n, piece, cols), bf16),
            dma((2, 3)), dma((3,)), dma((2, 3)), dma((CHUNKS,)), dma((3,)), dma((tp,)),
            dma((n // 2,)), dma((n // 2,)),
            dma((n, CHUNKS)), dma((CHUNKS,)), dma((n, CHUNKS)), dma((n, CHUNKS)), dma((1,)), dma((1,)),
            dma((2 * tp,)), dma((2 * tp,)), dma((8,)),
            dma((n, 2)), dma((n, 2)), dma((n,)), dma((n,)),
        ],
        compiler_params=pltpu.CompilerParams(
            collective_id=0, has_side_effects=True, vmem_limit_bytes=60 * 1024 * 1024
        ),
    )(
        lambdas, queries, keys, values, head_gain.reshape(1, -1), up_weight, down_weight,
        tokens, mixer_gain.reshape(1, -1), out_weight,
    )


def solution(mesh):
    placed = (
        P(("sp", "tp"), None),
        P("sp", "tp"),
        P("sp", "tp"),
        P("sp", "tp"),
        P("tp"),
        P(),
        P(),
        P(),
        P("sp", "tp"),
        P("tp", "sp"),
    )
    return jax.shard_map(
        functools.partial(per_device, mesh.shape["sp"], mesh.shape["tp"]),
        mesh=mesh,
        in_specs=placed,
        out_specs=P(("sp", "tp"), None),
        check_vma=False,
    )
```

```python
import functools

import jax
import jax.numpy as jnp
from jax import lax
from jax.experimental import pallas as pl
from jax.experimental.pallas import tpu as pltpu
from jax.sharding import PartitionSpec as P

DQK = 64
MESH = pl.DeviceIdType.MESH
f32, bf16 = jnp.float32, jnp.bfloat16
CHUNKS = 4
UPS, DOWNS = (0, 1), (2, 3)


def layer_kernel(
    n, tp,
    lam_ref, q_ref, k_ref, v_ref, gain_ref, up_ref, dn_ref, tok_ref, mix_ref, ow_hbm,
    out_ref,
    ah, upf_ref, dnf_ref,
    qb, kv, qm, run_max, run_sum, acc, att, att_above, ow, tokall, normed, hsum, hid, part, core_in, cross, cross_in,
    ex_send, ex_recv, top_recv, swap_send, tk_send, tk_recv, kv_send, kv_recv,
    w_send, own_send, y_send, w_recv, u_send, u_recv, a_send, a_recv, loc,
    c_send, c_recv, x_send, x_recv,
):
    s = lax.axis_index("sp")
    t = lax.axis_index("tp")
    z, y = s // 2, lax.rem(s, 2)
    x, c = t // 2, lax.rem(t, 2)
    steps = n // 2
    rows = q_ref.shape[0]
    wide = q_ref.shape[1] // 2
    total = 2 * rows
    piece = rows // tp
    top, helper = z == steps - 1, z == steps - 2
    has_up, has_down = z < steps - 1, z > 0
    above, below = (s + 2, t), (s - 2, t)
    beside = (s + 1 - 2 * y, t)
    core = (s, t + 1 - 2 * c)
    across_x = (s, lax.rem(t + 2, tp))
    line = 2 * z + c
    own_line = y == c
    partner = (line, 2 * x + y)

    barrier = pltpu.get_barrier_semaphore()

    def greet(device):
        pl.semaphore_signal(barrier, inc=1, device_id=device, device_id_type=MESH)

    for e in range(2):
        for i in range(tp):
            who = (2 * z + e, i)

            @pl.when(jnp.logical_or(e != y, i != t))
            def _():
                greet(who)

    pl.when(has_up)(lambda: greet(above))
    pl.when(has_down)(lambda: greet(below))
    pl.semaphore_wait(barrier, 2 * tp - 1 + has_up.astype(jnp.int32) + has_down.astype(jnp.int32))

    def remote(src, dst, send, recv, device):
        return pltpu.make_async_remote_copy(
            src_ref=src, dst_ref=dst, send_sem=send, recv_sem=recv, device_id=device, device_id_type=MESH
        )

    def rows_of(e):
        return pl.ds(pl.multiple_of(e * rows, rows), rows)

    def cols_of(e):
        return pl.ds(pl.multiple_of(e * wide, wide), wide)

    my_rows, peer_rows = rows_of(y), rows_of(1 - y)
    my_cols, peer_cols = cols_of(y), cols_of(1 - y)
    qkv = (q_ref, k_ref, v_ref)

    def landing(i, plane, slot, where):
        return qb.at[slot, where] if i == 0 else kv.at[plane, i - 1, where]

    def exchange(i, where):
        return remote(
            qkv[i].at[:, peer_cols], landing(i, z, 0, where), ex_send.at[0, i], ex_recv.at[i], beside
        )

    def lower(i, e):
        where = my_rows if e == 0 else peer_rows
        src = qkv[i].at[:, my_cols] if e == 0 else landing(i, z, 0, where)
        return remote(src, landing(i, z, 1, where), ex_send.at[1 + e, i], top_recv.at[y if e == 0 else 1 - y, i], below)

    def kv_part(j, r, i):
        part_of = kv.at[j, i, rows_of(r)]
        return remote(part_of, part_of, kv_send.at[j, r, i], kv_recv.at[j, r, i], above)

    def own_kv(i):
        return remote(
            qkv[1 + i].at[:, my_cols], kv.at[z, i, my_rows], kv_send.at[z, y, i], kv_recv.at[z, y, i], above
        )

    kv_rises = z < steps - 2
    for i in (1, 2, 0):
        exchange(i, my_rows).start()

    @pl.when(kv_rises)
    def _():
        for i in range(2):
            own_kv(i).start()

    @pl.when(top)
    def _():
        for i in range(3):
            lower(i, 0).start()

    depth, units = up_ref.shape
    half_depth, half = depth // 2, units // 2

    def shard(k, j):
        if k in UPS:
            return upf_ref.at[pl.ds(pl.multiple_of(j * depth + k * half_depth, half_depth), half_depth)]
        return dnf_ref.at[j, slice((k - 2) * half, (k - 1) * half)]

    given = (
        up_ref.at[slice(0, half_depth)], up_ref.at[slice(half_depth, depth)],
        dn_ref.at[slice(0, half)], dn_ref.at[slice(half, units)],
    )

    def swap(k):
        return remote(given[k], shard(k, s), swap_send.at[k], w_recv.at[s, k], partner)

    def send_above(k, j, src):
        remote(src, shard(k, j), w_send.at[j, k], w_recv.at[j, k], above).start()

    def send_below(k, j, src, sems):
        remote(src, shard(k, j), sems, w_recv.at[j, k], below).start()

    def over(k, j, src):
        remote(src, shard(k, j), y_send.at[j, k], w_recv.at[j, k], core).start()

    early_down = jnp.logical_or(z == 0, helper)

    def own_above(k, src):
        pl.when(has_up)(lambda: send_above(k, line, src))

    def own_around(k, src):
        pl.when(has_down)(lambda: send_below(k, line, src, own_send.at[k]))
        over(k, line, src)

    @pl.when(own_line)
    def _():
        for k in UPS:
            own_above(k, given[k])
            pl.when(jnp.logical_not(top))(lambda: own_around(k, given[k]))

    @pl.when(jnp.logical_not(own_line))
    def _():
        for k in UPS + DOWNS:
            swap(k).start()

    def band(i):
        return pl.ds(pl.multiple_of(i * piece, piece), piece)

    b = 2 * y + x
    bx = b + 1 - 2 * x
    by = lax.rem(b + 2, tp)
    bd = lax.rem(bx + 2, tp)

    half_piece = piece // 2

    def token_own(k):
        return remote(tok_ref, tokall.at[band(b)], tk_send.at[k], tk_recv.at[k], (across_x, beside)[k])

    def token_half(k):
        source = (bx, by)[k]
        moved = tokall.at[pl.ds(pl.multiple_of(source * piece + k * half_piece, half_piece), half_piece)]
        return remote(moved, moved, tk_send.at[2 + k], tk_recv.at[2 + k], (beside, across_x)[k])

    token_own(0).start()

    def local_copy(i):
        src, dst = (
            (k_ref.at[:, my_cols], kv.at[z, 0, my_rows]),
            (v_ref.at[:, my_cols], kv.at[z, 1, my_rows]),
            (q_ref.at[:, my_cols], qb.at[0, my_rows]),
            (up_ref, upf_ref.at[pl.ds(pl.multiple_of(s * depth, depth), depth)]),
            (dn_ref, dnf_ref.at[s]),
            (ow_hbm, ow),
            (tok_ref, tokall.at[band(b)]),
        )[i]
        return pltpu.make_async_copy(src, dst, loc.at[i])

    for i in range(3):
        local_copy(i).start()

    @pl.when(own_line)
    def _():
        local_copy(3).start()
        local_copy(4).start()

    local_copy(5).start()
    local_copy(6).start()

    for i in range(3):
        local_copy(i).wait()
    for i in (1, 2, 0):
        exchange(i, peer_rows).wait_recv()
        if i > 0:
            pl.when(kv_rises)(lambda: kv_part(z, 1 - y, i - 1).start())

    @pl.when(top)
    def _():
        for i in range(3):
            lower(i, 1).start()

    @pl.when(own_line)
    def _():
        for k in UPS:
            pl.when(top)(lambda: own_around(k, given[k]))
        for k in DOWNS:
            pl.when(early_down)(lambda: own_above(k, given[k]))
            own_around(k, given[k])

    def await_chunk(k, j):
        moved = shard(k, j)
        remote(moved, moved, w_send.at[j, k], w_recv.at[j, k], core).wait_recv()

    def from_core(k, i):
        await_chunk(k, 2 * i + 1 - c)

    def swapped(ks):
        @pl.when(jnp.logical_not(own_line))
        def _():
            for k in ks:
                await_chunk(k, line)
                src = shard(k, line)
                if k in UPS:
                    own_above(k, src)
                else:
                    pl.when(early_down)(lambda: own_above(k, src))
                own_around(k, src)

    def late_down():
        @pl.when(own_line)
        def _():
            for k in DOWNS:
                own_above(k, given[k])

        @pl.when(jnp.logical_not(own_line))
        def _():
            for k in DOWNS:
                own_above(k, shard(k, line))

    def from_above(d, ks):
        j = line + 2 * d
        for k in ks:
            await_chunk(k, j)
            src = shard(k, j)
            pl.when(has_down)(lambda: send_below(k, j, src, w_send.at[j, k]))
            over(k, j, src)

    def from_below(d, ks):
        j = line - 2 * d
        for k in ks:
            await_chunk(k, j)
            src = shard(k, j)
            pl.when(has_up)(lambda: send_above(k, j, src))
            over(k, j, src)

    chunk = min(512, total)
    lane = lax.broadcasted_iota(jnp.int32, (total, wide), 1)

    def weigh(sc, top_row):
        parts, whole = [], None
        for i in range(sc.shape[1] // 128):
            p = jnp.exp(sc[:, i * 128:(i + 1) * 128] - top_row)
            whole = p if whole is None else whole + p
            parts.append(p.astype(bf16))
        return jnp.concatenate(parts, axis=1), whole

    def scores_of(u, r0, j, keys):
        return lax.dot_general(
            qm[u, pl.ds(r0, chunk), :], kv[j, 0, :keys, :], (((1,), (1,)), ((), ())), preferred_element_type=f32
        )

    def diagonal(u, carry):
        @pl.when(u == 1)
        def _():
            for e in range(2):
                for i in range(3):
                    dst = landing(i, z + 1, 1, rows_of(e))
                    remote(dst, dst, ex_send.at[0, i], top_recv.at[e, i], above).wait_recv()

        scaled = qb[u] * jnp.asarray(DQK ** -0.5, bf16)
        for m in range(2):
            qm[u, m * total:(m + 1) * total, :] = jnp.where((lane < DQK) == (m == 0), scaled, jnp.zeros_like(scaled))
        j = z + u
        for m in range(2):
            for i in range(total // chunk):
                r0, keys = m * total + i * chunk, (i + 1) * chunk
                here = pl.ds(r0, chunk)
                sc = scores_of(u, r0, j, keys)
                qpos = i * chunk + lax.broadcasted_iota(jnp.int32, (chunk, keys), 0)
                kpos = lax.broadcasted_iota(jnp.int32, (chunk, keys), 1)
                sc = jnp.where(kpos <= qpos, sc, -jnp.inf)
                top_row = jnp.broadcast_to(jnp.max(sc, axis=1, keepdims=True), (chunk, 128))
                p, whole = weigh(sc, top_row)
                run_max[u, here, :] = top_row
                run_sum[u, here, :] = whole
                acc[u, here, :] = jnp.dot(p, kv[j, 1, :keys, :], preferred_element_type=f32)
        return carry

    def tiles(u, j):
        def tile(i, carry):
            r0 = pl.multiple_of(i * chunk, chunk)
            here = pl.ds(r0, chunk)
            sc = scores_of(u, r0, j, total)
            old = run_max[u, here, :]
            top_row = jnp.maximum(old, jnp.max(sc, axis=1, keepdims=True))
            p, whole = weigh(sc, top_row)
            shrink = jnp.exp(old - top_row)
            run_max[u, here, :] = top_row
            run_sum[u, here, :] = run_sum[u, here, :] * shrink + whole
            acc[u, here, :] = acc[u, here, :] * shrink + jnp.dot(p, kv[j, 1], preferred_element_type=f32)
            return carry

        lax.fori_loop(0, 2 * total // chunk, tile, 0)

    def finish(u, dst):
        lam = lam_ref[y]
        maps = []
        for m in range(2):
            here = slice(m * total, (m + 1) * total)
            maps.append(acc[u, here, :] / jnp.sum(run_sum[u, here, :], axis=1, keepdims=True))
        differ = maps[0] - lam * maps[1]
        spread = lax.rsqrt(jnp.mean(differ * differ, axis=1, keepdims=True) + 1e-06)
        dst[...] = (differ * spread * gain_ref[...]).astype(bf16).reshape(dst.shape)

    def raise_att():
        return remote(att_above, att, u_send.at[0], u_recv.at[0], above)

    @pl.when(jnp.logical_not(top))
    def _():
        diagonal(0, 0)

    swapped(UPS)

    @pl.when(helper)
    def _():
        lax.fori_loop(1, 2, diagonal, 0)
        swapped(DOWNS)
        tiles(1, z)

    def spread():
        pl.when(jnp.logical_not(helper))(lambda: swapped(DOWNS))

        @pl.when(own_line)
        def _():
            for k in DOWNS:
                from_core(k, z)

        token_own(1).start()
        token_own(0).wait_recv()
        token_half(0).start()

    middle = jnp.logical_and(z > 0, kv_rises)
    def pass_tokens():
        token_own(1).wait_recv()
        token_half(1).start()

    pl.when(jnp.logical_not(middle))(spread)

    def block(d, carry):
        j = z - d
        for r in (y, 1 - y):
            for i in range(2):
                kv_part(j, r, i).wait_recv()
                pl.when(kv_rises)(lambda: kv_part(j, r, i).start())

        pl.when(d == jnp.where(helper, 1, 2))(lambda: from_below(1, UPS))

        def slot(v, inner):
            u = 1 - v
            own_turn = jnp.logical_and(u == 0, d == 1)
            pl.when(jnp.logical_and(own_turn, helper))(lambda: from_above(1, UPS))
            tiles(u, j)

            @pl.when(jnp.logical_and(u == 1, d == z))
            def _():
                finish(1, att_above)
                raise_att().start()

            return inner

        lax.fori_loop(jnp.where(helper, 0, 1), 2, slot, 0)
        pl.when(jnp.logical_and(d == 1, middle))(spread)
        pl.when(jnp.logical_and(d == 1, kv_rises))(lambda: from_above(1, UPS))
        pl.when(d == 2)(lambda: from_above(1, DOWNS))
        return carry

    lax.fori_loop(1, jnp.where(top, 1, z + 1), block, 0)
    pl.when(jnp.logical_not(top))(lambda: finish(0, att))

    @pl.when(top)
    def _():
        from_below(1, UPS)
        pass_tokens()
        from_below(1, DOWNS)
        from_below(2, UPS)
        raise_att().wait_recv()

    head = 2 * t + y

    def head_cols(i):
        return pl.ds(pl.multiple_of(i * wide, wide), wide)

    def to_tokens(e, i, owner):
        return remote(
            att.at[:, i % 2], ah.at[:, :, head_cols(owner)], a_send.at[e * tp + i], a_recv.at[owner], (2 * z + e, i)
        )

    mine = pltpu.make_async_copy(att.at[:, c], ah.at[:, :, head_cols(head)], loc.at[7])
    mine.start()
    for e in range(2):
        for i in range(tp):
            pl.when(jnp.logical_or(e != y, i != t))(lambda: to_tokens(e, i, head).start())

    @pl.when(z == 0)
    def _():
        from_above(1, UPS + DOWNS)
        pass_tokens()

    @pl.when(z == 1)
    def _():
        from_below(1, UPS)
        late_down()
        from_above(1, DOWNS[:1])
        pass_tokens()
        from_above(2, UPS)
        from_above(1, DOWNS[1:])

    @pl.when(jnp.logical_and(z >= 2, has_up))
    def _():
        pass_tokens()
        from_below(2, UPS)
        pl.when(helper)(lambda: from_below(1, DOWNS))

    @pl.when(top)
    def _():
        from_below(3, UPS)

    local_copy(5).wait()
    local_copy(6).wait()
    mine.wait()
    for k in range(2):
        token_half(k).wait_recv()
        token_half(k).wait_send()
    for i in range(2 * tp):
        e, who = i % 2, i // 2
        pl.when(jnp.logical_or(e != y, who != t))(lambda: to_tokens(0, 0, i).wait_recv())

    def project(i, carry):
        span = pl.ds(pl.multiple_of(2 * i * piece, 2 * piece), 2 * piece)
        heads = ah[pl.ds(2 * i, 2)].reshape(2 * piece, 2 * tp * wide)
        projected = jnp.dot(heads, ow[...], preferred_element_type=f32).astype(bf16)
        summed = (tokall[span, :].astype(f32) + projected.astype(f32)).astype(bf16)
        tokall[span, :] = summed
        summed = summed.astype(f32)
        scale = lax.rsqrt(jnp.mean(summed * summed, axis=1, keepdims=True) + 1e-06)
        normed[span, :] = (summed * scale * mix_ref[...]).astype(bf16)
        return carry

    lax.fori_loop(0, tp // 2, project, 0)

    def later_ups(d, carry):
        pl.when(jnp.logical_and(z + d < steps, jnp.logical_or(z != 1, d != 2)))(lambda: from_above(d, UPS))
        waits = jnp.logical_and(d >= 3, jnp.logical_not(jnp.logical_and(top, d == 3)))
        pl.when(jnp.logical_and(z - d >= 0, waits))(lambda: from_below(d, UPS))
        return carry

    lax.fori_loop(2, steps, later_ups, 0)
    pl.when(jnp.logical_and(z > 1, kv_rises))(late_down)
    pl.when(jnp.logical_and(z >= 1, kv_rises))(lambda: from_below(1, DOWNS))

    @pl.when(own_line)
    def _():
        local_copy(3).wait()
        local_copy(4).wait()

    def order(k):
        return jnp.where(k < steps - z, z + k, steps - 1 - k)

    pair_depth = 2 * depth
    hsum[...] = jnp.zeros_like(hsum)

    def up_pair(k, carry):
        i = order(k)
        for m in UPS:
            from_core(m, i)
        span = pl.ds(pl.multiple_of(i * pair_depth, pair_depth), pair_depth)
        hsum[...] += jnp.dot(normed[:, span], upf_ref[span, :], preferred_element_type=f32)
        return carry

    lax.fori_loop(0, steps, up_pair, 0)
    hid[...] = jnp.square(jnp.maximum(hsum[...], 0.0)).astype(bf16)

    first = ((across_x, bx), (beside, by))

    def to_first(j, e, m):
        device, where = first[e]
        return remote(
            part.at[j, band(where if m == 0 else bd)], core_in.at[j, m], c_send.at[j, m], c_recv.at[j, m], device
        )

    def to_second(j, e):
        return remote(cross.at[j], cross_in.at[j], x_send.at[j], x_recv.at[j], first[1 - e][0])

    def relay(i):
        for e in range(2):
            j = 2 * i + e
            to_first(j, e, 1).wait_recv()
            where = first[1 - e][1]
            cross[j] = (part[j, band(where), :].astype(f32) + core_in[j, 1].astype(f32)).astype(bf16)
            to_second(j, e).start()

    def down_pair(k, carry):
        i = order(k)
        early = jnp.logical_and(k == steps - 1, jnp.logical_or(top, z == 0))

        @pl.when(early)
        def _():
            relay(order(k - 2))
            relay(order(k - 1))

        pl.when(i - z >= 2)(lambda: from_above(i - z, DOWNS))
        pl.when(z - i >= jnp.where(helper, 3, 2))(lambda: from_below(z - i, DOWNS))
        for m in DOWNS:
            pl.when(jnp.logical_and(helper, k == m - 1))(lambda: from_below(2, (m,)))
        for m in DOWNS:
            pl.when(jnp.logical_not(jnp.logical_and(own_line, i == z)))(lambda: from_core(m, i))
        for e in range(2):
            j = 2 * i + e
            part[j] = jnp.dot(hid[...], dnf_ref[j], preferred_element_type=f32).astype(bf16)
            to_first(j, e, 1).start()
            to_first(j, e, 0).start()
        pl.when(jnp.logical_and(k > 1, jnp.logical_not(early)))(lambda: relay(order(k - 2)))
        return carry

    lax.fori_loop(0, steps, down_pair, 0)
    pl.when(jnp.logical_not(jnp.logical_or(top, z == 0)))(lambda: relay(order(steps - 2)))
    relay(order(steps - 1))

    cols = dn_ref.shape[1]
    for j in reversed(range(n)):
        to_first(j, j % 2, 0).wait_recv()
        to_second(j, j % 2).wait_recv()
        here = slice(j * cols, (j + 1) * cols)
        both = part[j, band(b), :].astype(f32) + core_in[j, 0].astype(f32) + cross_in[j].astype(f32)
        out_ref[:, here] = (tokall[band(b), here].astype(f32) + both).astype(bf16)

    for j in range(n):
        to_first(j, j % 2, 0).wait_send()
        to_first(j, j % 2, 1).wait_send()
        to_second(j, j % 2).wait_send()
    for k in range(2):
        token_own(k).wait_send()
    for e in range(2):
        for i in range(tp):
            pl.when(jnp.logical_or(e != y, i != t))(lambda: to_tokens(e, i, head).wait_send())

    for i in range(3):
        exchange(i, my_rows).wait_send()

    @pl.when(top)
    def _():
        for i in range(3):
            for e in range(2):
                lower(i, e).wait_send()

    @pl.when(jnp.logical_not(own_line))
    def _():
        for k in UPS + DOWNS:
            swap(k).wait_send()

    pl.when(helper)(lambda: raise_att().wait_send())

    @pl.when(kv_rises)
    def _():
        def sent(j, carry):
            for r in range(2):
                for i in range(2):
                    kv_part(j, r, i).wait_send()
            return carry

        lax.fori_loop(0, z + 1, sent, 0)

    def line_sent(i, carry):
        j = 2 * i + c
        for k in UPS + DOWNS:
            moved = shard(k, j)
            remote(moved, moved, y_send.at[j, k], w_recv.at[j, k], core).wait_send()
            gone = jnp.logical_or(jnp.logical_and(i <= z, has_up), jnp.logical_and(i > z, has_down))
            pl.when(gone)(lambda: remote(moved, moved, w_send.at[j, k], w_recv.at[j, k], core).wait_send())
        return carry

    lax.fori_loop(0, steps, line_sent, 0)

    @pl.when(has_down)
    def _():
        for k in UPS + DOWNS:
            moved = shard(k, line)
            remote(moved, moved, own_send.at[k], w_recv.at[line, k], core).wait_send()


def per_device(
    n, tp, tokens, queries, keys, values, lambdas, head_gain, out_weight, mixer_gain, up_weight, down_weight
):
    rows, wide = queries.shape[0], queries.shape[1] // 2
    depth, units = up_weight.shape
    cols = down_weight.shape[1]
    piece, width = tokens.shape
    total = 2 * rows
    vmem = pl.BlockSpec(memory_space=pltpu.VMEM)
    dma = pltpu.SemaphoreType.DMA
    return pl.pallas_call(
        functools.partial(layer_kernel, n, tp),
        out_shape=jax.ShapeDtypeStruct(tokens.shape, bf16),
        in_specs=[pl.BlockSpec(memory_space=pltpu.SMEM)] + [vmem] * 8 + [pl.BlockSpec(memory_space=pl.ANY)],
        out_specs=vmem,
        scratch_shapes=[
            pltpu.VMEM((tp, piece, 2 * tp * wide), bf16),
            pltpu.VMEM((n * depth, units), bf16),
            pltpu.VMEM((n, units, cols), bf16),
            pltpu.VMEM((2, total, wide), bf16),
            pltpu.VMEM((n // 2, 2, total, wide), bf16),
            pltpu.VMEM((2, 2 * total, wide), bf16),
            pltpu.VMEM((2, 2 * total, 128), f32),
            pltpu.VMEM((2, 2 * total, 128), f32),
            pltpu.VMEM((2, 2 * total, wide), f32),
            pltpu.VMEM((tp, 2, piece, wide), bf16),
            pltpu.VMEM((tp, 2, piece, wide), bf16),
            pltpu.VMEM(out_weight.shape, bf16),
            pltpu.VMEM((rows, width), bf16),
            pltpu.VMEM((rows, width), bf16),
            pltpu.VMEM((rows, units), f32),
            pltpu.VMEM((rows, units), bf16),
            pltpu.VMEM((n, rows, cols), bf16),
            pltpu.VMEM((n, 2, piece, cols), bf16),
            pltpu.VMEM((n, piece, cols), bf16),
            pltpu.VMEM((n, piece, cols), bf16),
            dma((3, 3)), dma((3,)), dma((2, 3)), dma((CHUNKS,)), dma((4,)), dma((4,)),
            dma((n // 2, 2, 2)), dma((n // 2, 2, 2)),
            dma((n, CHUNKS)), dma((CHUNKS,)), dma((n, CHUNKS)), dma((n, CHUNKS)), dma((1,)), dma((1,)),
            dma((2 * tp,)), dma((2 * tp,)), dma((8,)),
            dma((n, 2)), dma((n, 2)), dma((n,)), dma((n,)),
        ],
        compiler_params=pltpu.CompilerParams(
            collective_id=0, has_side_effects=True, vmem_limit_bytes=60 * 1024 * 1024
        ),
    )(
        lambdas, queries, keys, values, head_gain.reshape(1, -1), up_weight, down_weight,
        tokens, mixer_gain.reshape(1, -1), out_weight,
    )


def solution(mesh):
    placed = (
        P(("sp", "tp"), None),
        P("sp", "tp"),
        P("sp", "tp"),
        P("sp", "tp"),
        P("tp"),
        P(),
        P(),
        P(),
        P("sp", "tp"),
        P("tp", "sp"),
    )
    return jax.shard_map(
        functools.partial(per_device, mesh.shape["sp"], mesh.shape["tp"]),
        mesh=mesh,
        in_specs=placed,
        out_specs=P(("sp", "tp"), None),
        check_vma=False,
    )
```

```python
import functools

import jax
import jax.numpy as jnp
from jax import lax
from jax.experimental import pallas as pl
from jax.experimental.pallas import tpu as pltpu
from jax.sharding import PartitionSpec as P

DQK = 64
MESH = pl.DeviceIdType.MESH
f32, bf16 = jnp.float32, jnp.bfloat16
CHUNKS = 4
UPS, DOWNS = (0, 1), (2, 3)


def layer_kernel(
    n, tp,
    lam_ref, gain_ref, mix_ref, q_hbm, k_hbm, v_hbm, up_hbm, dn_hbm, tok_hbm, ow_hbm,
    out_hbm,
    q_ref, k_ref, v_ref, up_ref, dn_ref, tok_ref,
    ah, upf_ref, dnf_ref,
    qb, kv, qm, run_max, run_sum, acc, att, ow, tokall, normed, hid, part, core_in, cross, cross_in, out_rows,
    ex_send, ex_recv, top_recv, swap_send, tk_send, tk_recv, kv_send, kv_recv,
    w_send, own_send, y_send, w_recv, u_send, u_recv, a_send, a_recv, loc, own_att, put_sem, in_sem,
    c_send, first_recv, c_recv, x_send, x_recv,
):
    s = lax.axis_index("sp")
    t = lax.axis_index("tp")
    z, y = s // 2, lax.rem(s, 2)
    x, c = t // 2, lax.rem(t, 2)
    steps = n // 2
    rows = q_ref.shape[0]
    wide = q_ref.shape[1] // 2
    total = 2 * rows
    piece = rows // tp
    top, helper = z == steps - 1, z == steps - 2
    has_up, has_down = z < steps - 1, z > 0
    above, below = (s + 2, t), (s - 2, t)
    beside = (s + 1 - 2 * y, t)
    core = (s, t + 1 - 2 * c)
    across_x = (s, lax.rem(t + 2, tp))
    line = 2 * z + c
    own_line = y == c
    partner = (line, 2 * x + y)

    fetched = []
    for i, (src, dst) in enumerate((
        (k_hbm, k_ref), (v_hbm, v_ref), (q_hbm, q_ref), (up_hbm, up_ref), (dn_hbm, dn_ref), (tok_hbm, tok_ref)
    )):
        fetched.append(pltpu.make_async_copy(src, dst, in_sem.at[i]))
        fetched[-1].start()

    barrier = pltpu.get_barrier_semaphore()

    def greet(device):
        pl.semaphore_signal(barrier, inc=1, device_id=device, device_id_type=MESH)

    for e in range(2):
        for i in range(tp):
            who = (2 * z + e, i)

            @pl.when(jnp.logical_or(e != y, i != t))
            def _():
                greet(who)

    pl.when(has_up)(lambda: greet(above))
    pl.when(has_down)(lambda: greet(below))
    pl.semaphore_wait(barrier, 2 * tp - 1 + has_up.astype(jnp.int32) + has_down.astype(jnp.int32))

    for copy in fetched:
        copy.wait()

    def remote(src, dst, send, recv, device):
        return pltpu.make_async_remote_copy(
            src_ref=src, dst_ref=dst, send_sem=send, recv_sem=recv, device_id=device, device_id_type=MESH
        )

    def drain(ref, sem):
        remote(ref, ref, sem, sem, beside).wait_send()

    def rows_of(e):
        return pl.ds(pl.multiple_of(e * rows, rows), rows)

    def cols_of(e):
        return pl.ds(pl.multiple_of(e * wide, wide), wide)

    my_rows, peer_rows = rows_of(y), rows_of(1 - y)
    my_cols, peer_cols = cols_of(y), cols_of(1 - y)
    qkv = (q_ref, k_ref, v_ref)

    def landing(i, plane, slot, where):
        return qb.at[slot, where] if i == 0 else kv.at[plane, i - 1, where]

    def exchange(i, where):
        return remote(
            qkv[i].at[:, peer_cols], landing(i, z, 0, where), ex_send.at[0], ex_recv.at[i], beside
        )

    def lower(i, e):
        where = my_rows if e == 0 else peer_rows
        src = qkv[i].at[:, my_cols] if e == 0 else landing(i, z, 0, where)
        return remote(src, landing(i, z, 1, where), ex_send.at[1 + e], top_recv.at[y if e == 0 else 1 - y], below)

    def kv_part(j, r, i):
        part_of = kv.at[j, i, rows_of(r)]
        return remote(part_of, part_of, kv_send.at[j], kv_recv.at[j, r], above)

    def own_kv(i):
        return remote(
            qkv[1 + i].at[:, my_cols], kv.at[z, i, my_rows], kv_send.at[z], kv_recv.at[z, y], above
        )

    kv_rises = z < steps - 2
    for i in (1, 2, 0):
        exchange(i, my_rows).start()

    @pl.when(kv_rises)
    def _():
        for i in range(2):
            own_kv(i).start()

    @pl.when(top)
    def _():
        for i in range(3):
            lower(i, 0).start()

    depth, units = up_ref.shape
    half_depth, half = depth // 2, units // 2

    def shard(k, j):
        if k in UPS:
            return upf_ref.at[pl.ds(pl.multiple_of(j * depth + k * half_depth, half_depth), half_depth)]
        return dnf_ref.at[j, slice((k - 2) * half, (k - 1) * half)]

    given = (
        up_ref.at[slice(0, half_depth)], up_ref.at[slice(half_depth, depth)],
        dn_ref.at[slice(0, half)], dn_ref.at[slice(half, units)],
    )

    def swap(k):
        return remote(given[k], shard(k, s), swap_send.at[0], w_recv.at[s, k], partner)

    def send_above(k, j, src):
        remote(src, shard(k, j), w_send.at[j], w_recv.at[j, k], above).start()

    def send_below(k, j, src, sems):
        remote(src, shard(k, j), sems, w_recv.at[j, k], below).start()

    def over(k, j, src):
        remote(src, shard(k, j), y_send.at[0], w_recv.at[j, k], core).start()

    early_down = jnp.logical_or(z == 0, helper)

    def own_above(k, src):
        pl.when(has_up)(lambda: send_above(k, line, src))

    def own_around(k, src):
        pl.when(has_down)(lambda: send_below(k, line, src, own_send.at[0]))
        over(k, line, src)

    @pl.when(own_line)
    def _():
        for k in UPS:
            own_above(k, given[k])
            pl.when(jnp.logical_not(top))(lambda: own_around(k, given[k]))
        for k in DOWNS:
            pl.when(helper)(lambda: own_above(k, given[k]))

    @pl.when(jnp.logical_not(own_line))
    def _():
        for k in UPS + DOWNS:
            swap(k).start()

    b = 2 * y + x
    bx = b + 1 - 2 * x
    by = lax.rem(b + 2, tp)
    bd = lax.rem(bx + 2, tp)

    half_piece = piece // 2

    def token_own(k):
        return remote(tok_ref, tokall.at[b], tk_send.at[k], tk_recv.at[k], (across_x, beside)[k])

    def token_half(k):
        source = (bx, by)[k]
        moved = tokall.at[source, pl.ds(k * half_piece, half_piece)]
        return remote(moved, moved, tk_send.at[2 + k], tk_recv.at[2 + k], (beside, across_x)[k])

    token_own(0).start()

    def local_copy(i):
        src, dst = (
            (k_ref.at[:, my_cols], kv.at[z, 0, my_rows]),
            (v_ref.at[:, my_cols], kv.at[z, 1, my_rows]),
            (q_ref.at[:, my_cols], qb.at[0, my_rows]),
            (up_ref, upf_ref.at[pl.ds(pl.multiple_of(s * depth, depth), depth)]),
            (dn_ref, dnf_ref.at[s]),
            (ow_hbm, ow),
            (tok_ref, tokall.at[b]),
        )[i]
        return pltpu.make_async_copy(src, dst, loc.at[i])

    for i in range(3):
        local_copy(i).start()

    @pl.when(own_line)
    def _():
        local_copy(3).start()
        local_copy(4).start()

    local_copy(5).start()
    local_copy(6).start()

    for i in range(3):
        local_copy(i).wait()
    for i in (1, 2, 0):
        exchange(i, peer_rows).wait_recv()
        if i > 0:
            pl.when(kv_rises)(lambda: kv_part(z, 1 - y, i - 1).start())

    @pl.when(top)
    def _():
        for i in range(3):
            lower(i, 1).start()

    @pl.when(own_line)
    def _():
        for k in UPS:
            pl.when(top)(lambda: own_around(k, given[k]))
        for k in DOWNS:
            pl.when(z == 0)(lambda: own_above(k, given[k]))
            own_around(k, given[k])

    def await_chunk(k, j):
        moved = shard(k, j)
        remote(moved, moved, w_send.at[j], w_recv.at[j, k], core).wait_recv()

    def from_core(k, i):
        await_chunk(k, 2 * i + 1 - c)

    def swapped(ks):
        @pl.when(jnp.logical_not(own_line))
        def _():
            for k in ks:
                await_chunk(k, line)
                src = shard(k, line)
                if k in UPS:
                    own_above(k, src)
                else:
                    pl.when(early_down)(lambda: own_above(k, src))
                own_around(k, src)

    def late_down():
        @pl.when(own_line)
        def _():
            for k in DOWNS:
                own_above(k, given[k])

        @pl.when(jnp.logical_not(own_line))
        def _():
            for k in DOWNS:
                own_above(k, shard(k, line))

    def from_above(d, ks):
        j = line + 2 * d
        for k in ks:
            await_chunk(k, j)
            src = shard(k, j)
            pl.when(has_down)(lambda: send_below(k, j, src, w_send.at[j]))
            over(k, j, src)

    def from_below(d, ks):
        j = line - 2 * d
        for k in ks:
            await_chunk(k, j)
            src = shard(k, j)
            pl.when(has_up)(lambda: send_above(k, j, src))
            over(k, j, src)

    chunk = rows
    lane = lax.broadcasted_iota(jnp.int32, (total, wide), 1)

    def weigh(sc, top_row):
        parts, whole = [], None
        for i in range(sc.shape[1] // 128):
            p = jnp.exp(sc[:, i * 128:(i + 1) * 128] - top_row)
            whole = p if whole is None else whole + p
            parts.append(p.astype(bf16))
        return jnp.concatenate(parts, axis=1), whole

    def scores_of(u, r0, j, keys):
        return lax.dot_general(
            qm[u, pl.ds(r0, chunk), :], kv[j, 0, :keys, :], (((1,), (1,)), ((), ())), preferred_element_type=f32
        )

    def diagonal(u, carry):
        @pl.when(u == 1)
        def _():
            for e in range(2):
                three = qm.at[1, slice(0, 3 * rows)]
                remote(three, three, ex_send.at[0], top_recv.at[e], above).wait_recv()

        scaled = qb[u] * jnp.asarray(DQK ** -0.5, bf16)
        for m in range(2):
            qm[u, m * total:(m + 1) * total, :] = jnp.where((lane < DQK) == (m == 0), scaled, jnp.zeros_like(scaled))
        j = z + u
        for m in range(2):
            for i in range(total // chunk):
                r0, keys = m * total + i * chunk, (i + 1) * chunk
                here = pl.ds(r0, chunk)
                sc = scores_of(u, r0, j, keys)
                qpos = i * chunk + lax.broadcasted_iota(jnp.int32, (chunk, keys), 0)
                kpos = lax.broadcasted_iota(jnp.int32, (chunk, keys), 1)
                sc = jnp.where(kpos <= qpos, sc, -jnp.inf)
                top_row = jnp.broadcast_to(jnp.max(sc, axis=1, keepdims=True), (chunk, 128))
                p, whole = weigh(sc, top_row)
                run_max[u, here, :] = top_row
                run_sum[u, here, :] = whole
                acc[u, here, :] = jnp.dot(p, kv[j, 1, :keys, :], preferred_element_type=f32)
        return carry

    def tile(u, j, r0):
        here = pl.ds(r0, chunk)
        sc = scores_of(u, r0, j, total)
        old = run_max[u, here, :]
        top_row = jnp.maximum(old, jnp.max(sc, axis=1, keepdims=True))
        p, whole = weigh(sc, top_row)
        shrink = jnp.exp(old - top_row)
        run_max[u, here, :] = top_row
        run_sum[u, here, :] = run_sum[u, here, :] * shrink + whole
        acc[u, here, :] = acc[u, here, :] * shrink + jnp.dot(p, kv[j, 1], preferred_element_type=f32)

    def tiles(u, j, hh):
        def one(m, carry):
            tile(u, j, pl.multiple_of(m * total + hh * rows, rows))
            return carry

        lax.fori_loop(0, 2, one, 0)

    def finish(u, hh):
        lam = lam_ref[y]
        maps = []
        for m in range(2):
            here = pl.ds(pl.multiple_of(m * total + hh * rows, rows), rows)
            maps.append(acc[u, here, :] / jnp.sum(run_sum[u, here, :], axis=1, keepdims=True))
        differ = maps[0] - lam * maps[1]
        spread_of = lax.rsqrt(jnp.mean(differ * differ, axis=1, keepdims=True) + 1e-06)
        done = (differ * spread_of * gain_ref[...]).astype(bf16)
        att[u, pl.ds(hh * (tp // 2), tp // 2)] = done.reshape(tp // 2, 2, piece, wide)

    def side(hh):
        return pl.ds(hh * (tp // 2), tp // 2)

    def raise_att(hh):
        return remote(att.at[1, side(hh)], att.at[0, side(hh)], u_send.at[hh], u_recv.at[hh], above)

    head = 2 * t + y

    def head_cols(i):
        return pl.ds(pl.multiple_of(i * wide, wide), wide)

    def to_tokens(hh, e, i, owner):
        return remote(
            att.at[0, side(hh), i % 2], ah.at[side(hh), :, head_cols(owner)],
            a_send.at[0], a_recv.at[0], (2 * z + e, i),
        )

    def mine(hh):
        return pltpu.make_async_copy(
            att.at[0, side(hh), c], ah.at[side(hh), :, head_cols(head)], own_att.at[hh]
        )

    def hand_out(hh):
        mine(hh).start()
        for e in range(2):
            for i in range(tp):
                pl.when(jnp.logical_or(e != y, i != t))(lambda: to_tokens(hh, e, i, head).start())

    def spread():
        swapped(DOWNS)

        @pl.when(own_line)
        def _():
            for k in DOWNS:
                from_core(k, z)

        token_own(1).start()
        token_own(0).wait_recv()
        token_half(0).start()

    def pass_tokens():
        token_own(1).wait_recv()
        token_half(1).start()

    @pl.when(jnp.logical_not(top))
    def _():
        diagonal(0, 0)

    swapped(UPS)
    forwarded = jnp.logical_and(helper, own_line)
    pl.when(forwarded)(lambda: from_below(1, UPS))

    @pl.when(helper)
    def _():
        lax.fori_loop(1, 2, diagonal, 0)
        spread()
        for hh in range(2):
            tiles(1, z, hh)

    middle = jnp.logical_and(z > 0, kv_rises)
    pl.when(jnp.logical_or(z == 0, top))(spread)

    def block(d, carry):
        j = z - d
        for r in (y, 1 - y):
            moved = kv.at[j, :, rows_of(r)]
            remote(moved, moved, kv_send.at[j], kv_recv.at[j, r], above).wait_recv()
            for i in range(2):
                pl.when(kv_rises)(lambda: kv_part(j, r, i).start())

        forward_now = jnp.logical_and(d == jnp.where(helper, 1, 2), jnp.logical_not(forwarded))
        pl.when(forward_now)(lambda: from_below(1, UPS))

        def slot(v, inner):
            u, hh = 1 - v // 2, lax.rem(v, 2)
            own_turn = jnp.logical_and(v == 2, helper)
            pl.when(jnp.logical_and(own_turn, d == 1))(lambda: from_above(1, UPS))
            pl.when(jnp.logical_and(own_turn, d == 2))(pass_tokens)
            tiles(u, j, hh)

            @pl.when(d == z)
            def _():
                finish(u, hh)
                pl.when(u == 1)(lambda: raise_att(hh).start())
                pl.when(u == 0)(lambda: hand_out(hh))

            return inner

        lax.fori_loop(jnp.where(helper, 0, 2), 4, slot, 0)
        pl.when(jnp.logical_and(d == 1, middle))(spread)
        pl.when(jnp.logical_and(d == 1, kv_rises))(lambda: from_above(1, UPS))
        pl.when(d == 2)(lambda: from_above(1, DOWNS))
        return carry

    lax.fori_loop(1, jnp.where(top, 1, z + 1), block, 0)

    @pl.when(z == 0)
    def _():
        for hh in range(2):
            finish(0, hh)
            hand_out(hh)

    @pl.when(top)
    def _():
        from_below(1, UPS)
        pass_tokens()
        from_below(1, DOWNS)
        from_below(2, UPS)
        for hh in range(2):
            raise_att(hh).wait_recv()
            hand_out(hh)

    @pl.when(z == 0)
    def _():
        from_above(1, UPS + DOWNS)
        pass_tokens()

    @pl.when(z == 1)
    def _():
        from_below(1, UPS)
        late_down()
        from_above(1, DOWNS[:1])
        pass_tokens()
        from_above(2, UPS)
        from_above(1, DOWNS[1:])

    @pl.when(jnp.logical_and(z >= 2, has_up))
    def _():
        pl.when(jnp.logical_not(helper))(pass_tokens)
        from_below(2, UPS)
        pl.when(helper)(lambda: from_below(1, DOWNS[:1]))

    @pl.when(top)
    def _():
        from_below(3, UPS)

    local_copy(5).wait()
    local_copy(6).wait()
    for hh in range(2):
        mine(hh).wait()
    for k in range(2):
        token_half(k).wait_recv()
        token_half(k).wait_send()
    others = ah.at[:, :, slice(0, (2 * tp - 1) * wide)]
    remote(others, others, a_send.at[0], a_recv.at[0], beside).wait_recv()

    def project(hf):
        part_rows = slice(hf * half_piece, (hf + 1) * half_piece)
        heads = ah[:, part_rows, :].reshape(2 * piece, 2 * tp * wide)
        projected = jnp.dot(heads, ow[...], preferred_element_type=f32).astype(bf16)
        given_tokens = tokall[:, part_rows, :].reshape(projected.shape).astype(f32)
        summed = (given_tokens + projected.astype(f32)).astype(bf16)
        tokall[:, part_rows, :] = summed.reshape(tp, half_piece, summed.shape[1])
        summed = summed.astype(f32)
        scale = lax.rsqrt(jnp.mean(summed * summed, axis=1, keepdims=True) + 1e-06)
        normed[hf] = (summed * scale * mix_ref[...]).astype(bf16)

    project(0)
    pl.when(helper)(lambda: from_below(1, DOWNS[1:]))

    def later_ups(d, carry):
        pl.when(jnp.logical_and(z + d < steps, jnp.logical_or(z != 1, d != 2)))(lambda: from_above(d, UPS))
        waits = jnp.logical_and(d >= 3, jnp.logical_not(jnp.logical_and(top, d == 3)))
        pl.when(jnp.logical_and(z - d >= 0, waits))(lambda: from_below(d, UPS))
        return carry

    lax.fori_loop(2, steps, later_ups, 0)
    pl.when(jnp.logical_and(z > 1, kv_rises))(late_down)
    pl.when(jnp.logical_and(z >= 1, kv_rises))(lambda: from_below(1, DOWNS))

    @pl.when(own_line)
    def _():
        local_copy(3).wait()
        local_copy(4).wait()

    def order(k):
        return jnp.where(k < steps - z, z + k, steps - 1 - k)

    def up_pair(k, carry):
        for m in UPS:
            from_core(m, k)
        return carry

    lax.fori_loop(0, steps, up_pair, 0)

    def unit(hf):
        inner = jnp.dot(normed[hf], upf_ref[...], preferred_element_type=f32)
        hid[hf] = jnp.square(jnp.maximum(inner, 0.0)).astype(bf16)

    first = ((across_x, bx), (beside, by))

    def to_first(j, e, m, hf):
        device, where = first[e]
        return remote(
            part.at[j, hf, where if m == 0 else bd], core_in.at[j, m, hf],
            c_send.at[0], (first_recv.at[j] if m == 0 else c_recv.at[j, hf]), device,
        )

    def to_second(j, e, hf):
        return remote(
            cross.at[j, hf], cross_in.at[j, hf], x_send.at[0], x_recv.at[j], first[1 - e][0]
        )

    def relay(i, hf):
        for e in range(2):
            j = 2 * i + e
            to_first(j, e, 1, hf).wait_recv()
            where = first[1 - e][1]
            cross[j, hf] = (part[j, hf, where].astype(f32) + core_in[j, 1, hf].astype(f32)).astype(bf16)
            to_second(j, e, hf).start()

    def multiply(i, hf):
        for e in range(2):
            j = 2 * i + e
            product = jnp.dot(hid[hf], dnf_ref[j], preferred_element_type=f32).astype(bf16)
            part[j, hf] = product.reshape(tp, half_piece, product.shape[1])
        for e in range(2):
            j = 2 * i + e
            to_first(j, e, 1, hf).start()
            to_first(j, e, 0, hf).start()

    def arrivals(k):
        i = order(k)
        pl.when(i - z >= 2)(lambda: from_above(i - z, DOWNS))
        pl.when(z - i >= jnp.where(helper, 3, 2))(lambda: from_below(z - i, DOWNS))
        for m in DOWNS:
            pl.when(jnp.logical_not(jnp.logical_and(own_line, i == z)))(lambda: from_core(m, i))

    ready = 2
    unit(0)

    def early_pair(k, carry):
        arrivals(k)
        multiply(order(k), 0)
        return carry

    lax.fori_loop(0, ready, early_pair, 0)
    project(1)
    unit(1)
    pl.when(helper)(lambda: from_below(2, DOWNS[:1]))

    def second_pair(k, carry):
        relay(order(k), 0)
        multiply(order(k), 1)
        return carry

    lax.fori_loop(0, ready, second_pair, 0)
    pl.when(helper)(lambda: from_below(2, DOWNS[1:]))
    edge = jnp.logical_or(top, z == 0)

    def relay_both(k):
        for hf in range(2):
            relay(order(k), hf)

    def late_pair(k, carry):
        final = k == steps - 1
        pl.when(jnp.logical_and(edge, final))(lambda: relay_both(k - 1))
        arrivals(k)
        for hf in range(2):
            multiply(order(k), hf)

        @pl.when(k == ready)
        def _():
            for i in range(ready):
                relay(order(i), 1)

        pl.when(jnp.logical_and(k > ready, jnp.logical_not(jnp.logical_and(edge, final))))(lambda: relay_both(k - 1))
        return carry

    lax.fori_loop(ready, steps, late_pair, 0)
    for k in range(2):
        token_own(k).wait_send()
    drain(others, a_send.at[0])
    three = qm.at[0, slice(0, 3 * rows)]
    drain(three, ex_send.at[0])

    @pl.when(top)
    def _():
        for e in range(2):
            drain(three, ex_send.at[1 + e])

    a_shard = upf_ref.at[slice(0, 2 * depth)]
    pl.when(jnp.logical_not(own_line))(lambda: drain(a_shard, swap_send.at[0]))

    @pl.when(helper)
    def _():
        for hh in range(2):
            raise_att(hh).wait_send()

    @pl.when(kv_rises)
    def _():
        def sent(j, carry):
            drain(kv.at[j], kv_send.at[j])
            return carry

        lax.fori_loop(0, z + 1, sent, 0)

    def line_sent(i, carry):
        gone = jnp.logical_or(jnp.logical_and(i <= z, has_up), jnp.logical_and(i > z, has_down))
        pl.when(gone)(lambda: drain(a_shard, w_send.at[2 * i + c]))
        return carry

    lax.fori_loop(0, steps, line_sent, 0)
    drain(upf_ref, y_send.at[0])
    pl.when(has_down)(lambda: drain(a_shard, own_send.at[0]))

    relay_both(steps - 1)
    cols = dn_ref.shape[1]
    width = out_hbm.shape[1]

    def put(i):
        here = slice(i * (width // 2), (i + 1) * (width // 2))
        return pltpu.make_async_copy(out_rows.at[:, here], out_hbm.at[:, here], put_sem.at[i])

    def close(js):
        for at, j in enumerate(js):
            mine_in = core_in.at[j, 0]
            remote(mine_in, mine_in, c_send.at[0], first_recv.at[j], beside).wait_recv()
            remote(cross_in.at[j], cross_in.at[j], x_send.at[0], x_recv.at[j], beside).wait_recv()
            here = slice(j * cols, (j + 1) * cols)
            both = part[j, :, b].astype(f32) + core_in[j, 0].astype(f32) + cross_in[j].astype(f32)
            out_rows[:, here] = (tokall[b, :, here].astype(f32) + both.reshape(piece, cols)).astype(bf16)
            if (at + 1) % (n // 2) == 0:
                put(j // (n // 2)).start()

    pl.when(z == 0)(lambda: close(tuple(range(n))))
    pl.when(z > 0)(lambda: close(tuple(range(n - 1, -1, -1))))

    drain(core_in, c_send.at[0])
    drain(cross, x_send.at[0])
    for i in range(2):
        put(i).wait()


def per_device(
    n, tp, tokens, queries, keys, values, lambdas, head_gain, out_weight, mixer_gain, up_weight, down_weight
):
    rows, wide = queries.shape[0], queries.shape[1] // 2
    depth, units = up_weight.shape
    cols = down_weight.shape[1]
    piece, width = tokens.shape
    total = 2 * rows
    vmem = pl.BlockSpec(memory_space=pltpu.VMEM)
    dma = pltpu.SemaphoreType.DMA
    return pl.pallas_call(
        functools.partial(layer_kernel, n, tp),
        out_shape=jax.ShapeDtypeStruct(tokens.shape, bf16),
        in_specs=[pl.BlockSpec(memory_space=pltpu.SMEM)] + [vmem] * 2 + [pl.BlockSpec(memory_space=pl.ANY)] * 7,
        out_specs=pl.BlockSpec(memory_space=pl.ANY),
        scratch_shapes=[
            pltpu.VMEM(queries.shape, bf16), pltpu.VMEM(keys.shape, bf16), pltpu.VMEM(values.shape, bf16),
            pltpu.VMEM(up_weight.shape, bf16), pltpu.VMEM(down_weight.shape, bf16), pltpu.VMEM(tokens.shape, bf16),
            pltpu.VMEM((tp, piece, 2 * tp * wide), bf16),
            pltpu.VMEM((n * depth, units), bf16),
            pltpu.VMEM((n, units, cols), bf16),
            pltpu.VMEM((2, total, wide), bf16),
            pltpu.VMEM((n // 2, 2, total, wide), bf16),
            pltpu.VMEM((2, 2 * total, wide), bf16),
            pltpu.VMEM((2, 2 * total, 128), f32),
            pltpu.VMEM((2, 2 * total, 128), f32),
            pltpu.VMEM((2, 2 * total, wide), f32),
            pltpu.VMEM((2, tp, 2, piece, wide), bf16),
            pltpu.VMEM(out_weight.shape, bf16),
            pltpu.VMEM((tp, piece, width), bf16),
            pltpu.VMEM((2, 2 * piece, width), bf16),
            pltpu.VMEM((2, 2 * piece, units), bf16),
            pltpu.VMEM((n, 2, tp, piece // 2, cols), bf16),
            pltpu.VMEM((n, 2, 2, piece // 2, cols), bf16),
            pltpu.VMEM((n, 2, piece // 2, cols), bf16),
            pltpu.VMEM((n, 2, piece // 2, cols), bf16),
            pltpu.VMEM((piece, width), bf16),
            dma((3,)), dma((3,)), dma((2,)), dma((1,)), dma((4,)), dma((4,)),
            dma((n // 2,)), dma((n // 2, 2)),
            dma((n,)), dma((1,)), dma((1,)), dma((n, CHUNKS)), dma((2,)), dma((2,)),
            dma((1,)), dma((1,)), dma((7,)), dma((2,)), dma((2,)), dma((6,)),
            dma((1,)), dma((n,)), dma((n, 2)), dma((1,)), dma((n,)),
        ],
        compiler_params=pltpu.CompilerParams(
            collective_id=0, has_side_effects=True, vmem_limit_bytes=60 * 1024 * 1024
        ),
    )(
        lambdas, head_gain.reshape(1, -1), mixer_gain.reshape(1, -1), queries, keys, values, up_weight, down_weight,
        tokens, out_weight,
    )


def solution(mesh):
    placed = (
        P(("sp", "tp"), None),
        P("sp", "tp"),
        P("sp", "tp"),
        P("sp", "tp"),
        P("tp"),
        P(),
        P(),
        P(),
        P("sp", "tp"),
        P("tp", "sp"),
    )
    return jax.shard_map(
        functools.partial(per_device, mesh.shape["sp"], mesh.shape["tp"]),
        mesh=mesh,
        in_specs=placed,
        out_specs=P(("sp", "tp"), None),
        check_vma=False,
    )
```

```python
import functools

import jax
import jax.numpy as jnp
from jax import lax
from jax.experimental import pallas as pl
from jax.experimental.pallas import tpu as pltpu
from jax.sharding import PartitionSpec as P

DQK = 64
MESH = pl.DeviceIdType.MESH
f32, bf16 = jnp.float32, jnp.bfloat16
CHUNKS = 4
UPS, DOWNS = (0, 1), (2, 3)


def layer_kernel(
    n, tp,
    lam_ref, gain_ref, mix_ref, q_hbm, k_hbm, v_hbm, up_hbm, dn_hbm, tok_hbm, ow_hbm,
    out_rows,
    q_ref, k_ref, v_ref, up_ref, dn_ref, tok_ref,
    ah, upf_ref, dnf_ref,
    qb, kv, qm, run_max, run_sum, acc, att, ow, tokall, normed, hid, part, core_in, cross, cross_in,
    ex_send, ex_recv, top_recv, swap_send, tk_send, tk_recv, kv_send, kv_recv,
    w_send, own_send, y_send, w_recv, u_send, u_recv, a_send, a_recv, loc, own_att, put_sem, in_sem,
    c_send, first_recv, c_recv, x_send, x_recv,
):
    s = lax.axis_index("sp")
    t = lax.axis_index("tp")
    z, y = s // 2, lax.rem(s, 2)
    x, c = t // 2, lax.rem(t, 2)
    steps = n // 2
    rows = q_ref.shape[0]
    wide = q_ref.shape[1] // 2
    total = 2 * rows
    piece = rows // tp
    top, helper = z == steps - 1, z == steps - 2
    has_up, has_down = z < steps - 1, z > 0
    above, below = (s + 2, t), (s - 2, t)
    beside = (s + 1 - 2 * y, t)
    core = (s, t + 1 - 2 * c)
    across_x = (s, lax.rem(t + 2, tp))
    line = 2 * z + c
    own_line = y == c
    partner = (line, 2 * x + y)

    fetched = []
    for i, (src, dst) in enumerate((
        (k_hbm, k_ref), (v_hbm, v_ref), (q_hbm, q_ref), (up_hbm, up_ref), (dn_hbm, dn_ref), (tok_hbm, tok_ref)
    )):
        fetched.append(pltpu.make_async_copy(src, dst, in_sem.at[i]))
        fetched[-1].start()

    barrier = pltpu.get_barrier_semaphore()

    def greet(device):
        pl.semaphore_signal(barrier, inc=1, device_id=device, device_id_type=MESH)

    for e in range(2):
        for i in range(tp):
            who = (2 * z + e, i)

            @pl.when(jnp.logical_or(e != y, i != t))
            def _():
                greet(who)

    pl.when(has_up)(lambda: greet(above))
    pl.when(has_down)(lambda: greet(below))
    pl.semaphore_wait(barrier, 2 * tp - 1 + has_up.astype(jnp.int32) + has_down.astype(jnp.int32))

    for copy in fetched:
        copy.wait()

    def remote(src, dst, send, recv, device):
        return pltpu.make_async_remote_copy(
            src_ref=src, dst_ref=dst, send_sem=send, recv_sem=recv, device_id=device, device_id_type=MESH
        )

    def drain(ref, sem):
        remote(ref, ref, sem, sem, beside).wait_send()

    def rows_of(e):
        return pl.ds(pl.multiple_of(e * rows, rows), rows)

    def cols_of(e):
        return pl.ds(pl.multiple_of(e * wide, wide), wide)

    my_rows, peer_rows = rows_of(y), rows_of(1 - y)
    my_cols, peer_cols = cols_of(y), cols_of(1 - y)
    qkv = (q_ref, k_ref, v_ref)

    def landing(i, plane, slot, where):
        return qb.at[slot, where] if i == 0 else kv.at[plane, i - 1, where]

    def exchange(i, where):
        return remote(
            qkv[i].at[:, peer_cols], landing(i, z, 0, where), ex_send.at[0], ex_recv.at[i], beside
        )

    def lower(i, e):
        where = my_rows if e == 0 else peer_rows
        src = qkv[i].at[:, my_cols] if e == 0 else landing(i, z, 0, where)
        return remote(src, landing(i, z, 1, where), ex_send.at[1 + e], top_recv.at[y if e == 0 else 1 - y], below)

    def kv_part(j, r, i):
        part_of = kv.at[j, i, rows_of(r)]
        return remote(part_of, part_of, kv_send.at[j], kv_recv.at[j, r], above)

    def own_kv(i):
        return remote(
            qkv[1 + i].at[:, my_cols], kv.at[z, i, my_rows], kv_send.at[z], kv_recv.at[z, y], above
        )

    kv_rises = z < steps - 2
    for i in (1, 2, 0):
        exchange(i, my_rows).start()

    @pl.when(kv_rises)
    def _():
        for i in range(2):
            own_kv(i).start()

    @pl.when(top)
    def _():
        for i in range(3):
            lower(i, 0).start()

    depth, units = up_ref.shape
    half_depth, half = depth // 2, units // 2

    def shard(k, j):
        if k in UPS:
            return upf_ref.at[pl.ds(pl.multiple_of(j * depth + k * half_depth, half_depth), half_depth)]
        return dnf_ref.at[j, slice((k - 2) * half, (k - 1) * half)]

    given = (
        up_ref.at[slice(0, half_depth)], up_ref.at[slice(half_depth, depth)],
        dn_ref.at[slice(0, half)], dn_ref.at[slice(half, units)],
    )

    def swap(k):
        return remote(given[k], shard(k, s), swap_send.at[0], w_recv.at[s, k], partner)

    def send_above(k, j, src):
        remote(src, shard(k, j), w_send.at[j], w_recv.at[j, k], above).start()

    def send_below(k, j, src, sems):
        remote(src, shard(k, j), sems, w_recv.at[j, k], below).start()

    def over(k, j, src):
        remote(src, shard(k, j), y_send.at[0], w_recv.at[j, k], core).start()

    early_down = jnp.logical_or(z == 0, helper)

    def own_above(k, src):
        pl.when(has_up)(lambda: send_above(k, line, src))

    def own_around(k, src):
        pl.when(has_down)(lambda: send_below(k, line, src, own_send.at[0]))
        over(k, line, src)

    @pl.when(own_line)
    def _():
        for k in UPS:
            own_above(k, given[k])
            pl.when(jnp.logical_not(top))(lambda: own_around(k, given[k]))
        for k in DOWNS:
            pl.when(helper)(lambda: own_above(k, given[k]))

    @pl.when(jnp.logical_not(own_line))
    def _():
        for k in UPS + DOWNS:
            swap(k).start()

    b = 2 * y + x
    bx = b + 1 - 2 * x
    by = lax.rem(b + 2, tp)
    bd = lax.rem(bx + 2, tp)

    half_piece = piece // 2

    def token_own(k):
        return remote(tok_ref, tokall.at[b], tk_send.at[k], tk_recv.at[k], (across_x, beside)[k])

    def token_half(k):
        source = (bx, by)[k]
        moved = tokall.at[source, pl.ds(k * half_piece, half_piece)]
        return remote(moved, moved, tk_send.at[2 + k], tk_recv.at[2 + k], (beside, across_x)[k])

    token_own(0).start()

    def local_copy(i):
        src, dst = (
            (k_ref.at[:, my_cols], kv.at[z, 0, my_rows]),
            (v_ref.at[:, my_cols], kv.at[z, 1, my_rows]),
            (q_ref.at[:, my_cols], qb.at[0, my_rows]),
            (up_ref, upf_ref.at[pl.ds(pl.multiple_of(s * depth, depth), depth)]),
            (dn_ref, dnf_ref.at[s]),
            (ow_hbm, ow),
            (tok_ref, tokall.at[b]),
        )[i]
        return pltpu.make_async_copy(src, dst, loc.at[i])

    for i in range(3):
        local_copy(i).start()

    @pl.when(own_line)
    def _():
        local_copy(3).start()
        local_copy(4).start()

    local_copy(5).start()
    local_copy(6).start()

    for i in range(3):
        local_copy(i).wait()
    for i in (1, 2, 0):
        exchange(i, peer_rows).wait_recv()
        if i > 0:
            pl.when(kv_rises)(lambda: kv_part(z, 1 - y, i - 1).start())

    @pl.when(top)
    def _():
        for i in range(3):
            lower(i, 1).start()

    @pl.when(own_line)
    def _():
        for k in UPS:
            pl.when(top)(lambda: own_around(k, given[k]))
        for k in DOWNS:
            pl.when(z == 0)(lambda: own_above(k, given[k]))
            own_around(k, given[k])

    def await_chunk(k, j):
        moved = shard(k, j)
        remote(moved, moved, w_send.at[j], w_recv.at[j, k], core).wait_recv()

    def from_core(k, i):
        await_chunk(k, 2 * i + 1 - c)

    def swapped(ks):
        @pl.when(jnp.logical_not(own_line))
        def _():
            for k in ks:
                await_chunk(k, line)
                src = shard(k, line)
                if k in UPS:
                    own_above(k, src)
                else:
                    pl.when(early_down)(lambda: own_above(k, src))
                own_around(k, src)

    def late_down():
        @pl.when(own_line)
        def _():
            for k in DOWNS:
                own_above(k, given[k])

        @pl.when(jnp.logical_not(own_line))
        def _():
            for k in DOWNS:
                own_above(k, shard(k, line))

    def from_above(d, ks):
        j = line + 2 * d
        for k in ks:
            await_chunk(k, j)
            src = shard(k, j)
            pl.when(has_down)(lambda: send_below(k, j, src, w_send.at[j]))
            over(k, j, src)

    def from_below(d, ks):
        j = line - 2 * d
        for k in ks:
            await_chunk(k, j)
            src = shard(k, j)
            pl.when(has_up)(lambda: send_above(k, j, src))
            over(k, j, src)

    chunk = rows
    lane = lax.broadcasted_iota(jnp.int32, (total, wide), 1)

    def weigh(sc, top_row):
        parts, whole = [], None
        for i in range(sc.shape[1] // 128):
            p = jnp.exp(sc[:, i * 128:(i + 1) * 128] - top_row)
            whole = p if whole is None else whole + p
            parts.append(p.astype(bf16))
        return jnp.concatenate(parts, axis=1), whole

    def scores_of(u, r0, j, keys):
        return lax.dot_general(
            qm[u, pl.ds(r0, chunk), :], kv[j, 0, :keys, :], (((1,), (1,)), ((), ())), preferred_element_type=f32
        )

    def diagonal(u, carry):
        @pl.when(u == 1)
        def _():
            for e in range(2):
                three = qm.at[1, slice(0, 3 * rows)]
                remote(three, three, ex_send.at[0], top_recv.at[e], above).wait_recv()

        scaled = qb[u] * jnp.asarray(DQK ** -0.5, bf16)
        for m in range(2):
            qm[u, m * total:(m + 1) * total, :] = jnp.where((lane < DQK) == (m == 0), scaled, jnp.zeros_like(scaled))
        j = z + u
        for m in range(2):
            for i in range(total // chunk):
                r0, keys = m * total + i * chunk, (i + 1) * chunk
                here = pl.ds(r0, chunk)
                sc = scores_of(u, r0, j, keys)
                qpos = i * chunk + lax.broadcasted_iota(jnp.int32, (chunk, keys), 0)
                kpos = lax.broadcasted_iota(jnp.int32, (chunk, keys), 1)
                sc = jnp.where(kpos <= qpos, sc, -jnp.inf)
                top_row = jnp.broadcast_to(jnp.max(sc, axis=1, keepdims=True), (chunk, 128))
                p, whole = weigh(sc, top_row)
                run_max[u, here, :] = top_row
                run_sum[u, here, :] = whole
                acc[u, here, :] = jnp.dot(p, kv[j, 1, :keys, :], preferred_element_type=f32)
        return carry

    def tile(u, j, r0):
        here = pl.ds(r0, chunk)
        sc = scores_of(u, r0, j, total)
        old = run_max[u, here, :]
        top_row = jnp.maximum(old, jnp.max(sc, axis=1, keepdims=True))
        p, whole = weigh(sc, top_row)
        shrink = jnp.exp(old - top_row)
        run_max[u, here, :] = top_row
        run_sum[u, here, :] = run_sum[u, here, :] * shrink + whole
        acc[u, here, :] = acc[u, here, :] * shrink + jnp.dot(p, kv[j, 1], preferred_element_type=f32)

    def tiles(u, j, hh):
        def one(m, carry):
            tile(u, j, pl.multiple_of(m * total + hh * rows, rows))
            return carry

        lax.fori_loop(0, 2, one, 0)

    def finish(u, hh):
        lam = lam_ref[y]
        maps = []
        for m in range(2):
            here = pl.ds(pl.multiple_of(m * total + hh * rows, rows), rows)
            maps.append(acc[u, here, :] / jnp.sum(run_sum[u, here, :], axis=1, keepdims=True))
        differ = maps[0] - lam * maps[1]
        spread_of = lax.rsqrt(jnp.mean(differ * differ, axis=1, keepdims=True) + 1e-06)
        done = (differ * spread_of * gain_ref[...]).astype(bf16)
        att[u, pl.ds(hh * (tp // 2), tp // 2)] = done.reshape(tp // 2, 2, piece, wide)

    def side(hh):
        return pl.ds(hh * (tp // 2), tp // 2)

    def raise_att(hh):
        return remote(att.at[1, side(hh)], att.at[0, side(hh)], u_send.at[hh], u_recv.at[hh], above)

    head = 2 * t + y

    def head_cols(i):
        return pl.ds(pl.multiple_of(i * wide, wide), wide)

    def to_tokens(hh, e, i, owner):
        return remote(
            att.at[0, side(hh), i % 2], ah.at[side(hh), :, head_cols(owner)],
            a_send.at[0], a_recv.at[0], (2 * z + e, i),
        )

    def mine(hh):
        return pltpu.make_async_copy(
            att.at[0, side(hh), c], ah.at[side(hh), :, head_cols(head)], own_att.at[hh]
        )

    def hand_out(hh):
        mine(hh).start()
        for e in range(2):
            for i in range(tp):
                pl.when(jnp.logical_or(e != y, i != t))(lambda: to_tokens(hh, e, i, head).start())

    def spread():
        swapped(DOWNS)

        @pl.when(own_line)
        def _():
            for k in DOWNS:
                from_core(k, z)

        token_own(1).start()

    def pass_tokens():
        for k in (1, 0):
            token_own(k).wait_recv()
            token_half(k).start()

    @pl.when(jnp.logical_not(top))
    def _():
        diagonal(0, 0)

    swapped(UPS)
    forwarded = jnp.logical_and(helper, own_line)
    pl.when(forwarded)(lambda: from_below(1, UPS))

    @pl.when(helper)
    def _():
        spread()
        lax.fori_loop(1, 2, diagonal, 0)
        for hh in range(2):
            tiles(1, z, hh)

    middle = jnp.logical_and(z > 0, kv_rises)
    pl.when(jnp.logical_or(z == 0, top))(spread)

    def block(d, carry):
        j = z - d
        for r in (y, 1 - y):
            moved = kv.at[j, :, rows_of(r)]
            remote(moved, moved, kv_send.at[j], kv_recv.at[j, r], above).wait_recv()
            for i in range(2):
                pl.when(kv_rises)(lambda: kv_part(j, r, i).start())

        forward_now = jnp.logical_and(d == jnp.where(helper, 1, 2), jnp.logical_not(forwarded))
        pl.when(forward_now)(lambda: from_below(1, UPS))

        @pl.when(jnp.logical_and(helper, d == 2))
        def _():
            pass_tokens()
            from_above(1, DOWNS[:1])


        def ahead():
            from_above(1, DOWNS[1:])
            from_below(2, UPS[:1])

        def slot(v, inner):
            u, hh = 1 - v // 2, lax.rem(v, 2)
            own_turn = jnp.logical_and(v == 2, helper)
            pl.when(jnp.logical_and(own_turn, d == 1))(lambda: from_above(1, UPS))
            pl.when(jnp.logical_and(helper, jnp.logical_and(v == 3, d == 2)))(ahead)
            tiles(u, j, hh)

            @pl.when(d == z)
            def _():
                finish(u, hh)
                pl.when(u == 1)(lambda: raise_att(hh).start())
                pl.when(u == 0)(lambda: hand_out(hh))

            return inner

        lax.fori_loop(jnp.where(helper, 0, 2), 4, slot, 0)
        pl.when(jnp.logical_and(d == 1, middle))(spread)
        pl.when(jnp.logical_and(d == 1, kv_rises))(lambda: from_above(1, UPS))
        pl.when(jnp.logical_and(d == 2, kv_rises))(lambda: from_above(1, DOWNS))
        return carry

    lax.fori_loop(1, jnp.where(top, 1, z + 1), block, 0)

    @pl.when(z == 0)
    def _():
        for hh in range(2):
            finish(0, hh)
            hand_out(hh)

    @pl.when(top)
    def _():
        from_below(1, UPS)
        pass_tokens()
        from_below(1, DOWNS)
        from_below(2, UPS)
        for hh in range(2):
            raise_att(hh).wait_recv()
            hand_out(hh)

    @pl.when(z == 0)
    def _():
        from_above(1, UPS + DOWNS)
        pass_tokens()

    @pl.when(z == 1)
    def _():
        pl.when(jnp.logical_not(forwarded))(lambda: from_below(1, UPS))
        late_down()
        from_above(1, DOWNS[:1])
        from_above(2, UPS)
        from_above(1, DOWNS[1:])
        pass_tokens()
        from_above(2, DOWNS)

    @pl.when(jnp.logical_and(z >= 2, has_up))
    def _():
        pl.when(jnp.logical_not(helper))(pass_tokens)
        pl.when(jnp.logical_not(helper))(lambda: from_below(2, UPS[:1]))
        from_below(2, UPS[1:])
        pl.when(helper)(lambda: from_below(1, DOWNS[:1]))

    @pl.when(top)
    def _():
        from_below(3, UPS)

    local_copy(5).wait()
    local_copy(6).wait()
    for hh in range(2):
        mine(hh).wait()
    for k in range(2):
        token_half(k).wait_recv()
        token_half(k).wait_send()
    others = ah.at[:, :, slice(0, (2 * tp - 1) * wide)]
    remote(others, others, a_send.at[0], a_recv.at[0], beside).wait_recv()

    def project(hf):
        part_rows = slice(hf * half_piece, (hf + 1) * half_piece)
        heads = ah[:, part_rows, :].reshape(2 * piece, 2 * tp * wide)
        projected = jnp.dot(heads, ow[...], preferred_element_type=f32).astype(bf16)
        given_tokens = tokall[:, part_rows, :].reshape(projected.shape).astype(f32)
        summed = (given_tokens + projected.astype(f32)).astype(bf16)
        tokall[:, part_rows, :] = summed.reshape(tp, half_piece, summed.shape[1])
        summed = summed.astype(f32)
        scale = lax.rsqrt(jnp.mean(summed * summed, axis=1, keepdims=True) + 1e-06)
        normed[hf] = (summed * scale * mix_ref[...]).astype(bf16)

    project(0)
    pl.when(helper)(lambda: from_below(1, DOWNS[1:]))

    def later_ups(d, carry):
        pl.when(jnp.logical_and(z + d < steps, jnp.logical_or(z != 1, d != 2)))(lambda: from_above(d, UPS))
        waits = jnp.logical_and(d >= 3, jnp.logical_not(jnp.logical_and(top, d == 3)))
        pl.when(jnp.logical_and(z - d >= 0, waits))(lambda: from_below(d, UPS))
        return carry

    lax.fori_loop(2, steps, later_ups, 0)
    pl.when(jnp.logical_and(z > 1, kv_rises))(late_down)
    pl.when(jnp.logical_and(z >= 1, kv_rises))(lambda: from_below(1, DOWNS))

    @pl.when(own_line)
    def _():
        local_copy(3).wait()
        local_copy(4).wait()

    def order(k):
        return jnp.where(k < steps - z, z + k, steps - 1 - k)

    def up_pair(k, carry):
        for m in UPS:
            from_core(m, k)
        return carry

    lax.fori_loop(0, steps, up_pair, 0)

    def unit(hf):
        inner = jnp.dot(normed[hf], upf_ref[...], preferred_element_type=f32)
        hid[hf] = jnp.square(jnp.maximum(inner, 0.0)).astype(bf16)

    first = ((across_x, bx), (beside, by))

    def to_first(j, e, m, hf):
        device, where = first[e]
        return remote(
            part.at[j, hf, where if m == 0 else bd], core_in.at[j, m, hf],
            c_send.at[0], (first_recv.at[j] if m == 0 else c_recv.at[j, hf]), device,
        )

    def to_second(j, e, hf):
        return remote(
            cross.at[j, hf], cross_in.at[j, hf], x_send.at[0], x_recv.at[j], first[1 - e][0]
        )

    def relay(i, hf):
        for e in range(2):
            j = 2 * i + e
            to_first(j, e, 1, hf).wait_recv()
            where = first[1 - e][1]
            cross[j, hf] = (part[j, hf, where].astype(f32) + core_in[j, 1, hf].astype(f32)).astype(bf16)
            to_second(j, e, hf).start()

    def multiply(i, hfs):
        for hf in hfs:
            for e in range(2):
                j = 2 * i + e
                product = jnp.dot(hid[hf], dnf_ref[j], preferred_element_type=f32).astype(bf16)
                part[j, hf] = product.reshape(tp, half_piece, product.shape[1])
            for e in range(2):
                to_first(2 * i + e, e, 1, hf).start()
        for hf in hfs:
            for e in range(2):
                to_first(2 * i + e, e, 0, hf).start()

    def arrivals(k):
        i = order(k)
        pl.when(i - z >= jnp.where(z == 1, 3, 2))(lambda: from_above(i - z, DOWNS))
        pl.when(z - i >= jnp.where(helper, 3, 2))(lambda: from_below(z - i, DOWNS))
        for m in DOWNS:
            pl.when(jnp.logical_not(jnp.logical_and(own_line, i == z)))(lambda: from_core(m, i))

    ready = 2
    unit(0)

    def early_pair(k, carry):
        arrivals(k)
        multiply(order(k), (0,))
        return carry

    lax.fori_loop(0, ready, early_pair, 0)
    project(1)
    unit(1)
    pl.when(helper)(lambda: from_below(2, DOWNS[:1]))

    def second_pair(k, carry):
        relay(order(k), 0)
        multiply(order(k), (1,))
        return carry

    lax.fori_loop(0, ready, second_pair, 0)
    pl.when(helper)(lambda: from_below(2, DOWNS[1:]))
    edge = jnp.logical_or(top, z == 0)

    def relay_both(k):
        for hf in range(2):
            relay(order(k), hf)

    def late_pair(k, carry):
        final = k == steps - 1
        pl.when(jnp.logical_and(edge, final))(lambda: relay_both(k - 1))
        arrivals(k)
        multiply(order(k), (0, 1))

        @pl.when(k == ready)
        def _():
            for i in range(ready):
                relay(order(i), 1)

        pl.when(jnp.logical_and(k > ready, jnp.logical_not(jnp.logical_and(edge, final))))(lambda: relay_both(k - 1))
        return carry

    lax.fori_loop(ready, steps, late_pair, 0)
    for k in range(2):
        token_own(k).wait_send()
    drain(others, a_send.at[0])
    three = qm.at[0, slice(0, 3 * rows)]
    drain(three, ex_send.at[0])

    @pl.when(top)
    def _():
        for e in range(2):
            drain(three, ex_send.at[1 + e])

    a_shard = upf_ref.at[slice(0, 2 * depth)]
    pl.when(jnp.logical_not(own_line))(lambda: drain(a_shard, swap_send.at[0]))

    @pl.when(helper)
    def _():
        for hh in range(2):
            raise_att(hh).wait_send()

    @pl.when(kv_rises)
    def _():
        def sent(j, carry):
            drain(kv.at[j], kv_send.at[j])
            return carry

        lax.fori_loop(0, z + 1, sent, 0)

    relay_both(steps - 1)
    cols = dn_ref.shape[1]
    def close(js):
        for at, j in enumerate(js):
            mine_in = core_in.at[j, 0]
            remote(mine_in, mine_in, c_send.at[0], first_recv.at[j], beside).wait_recv()
            remote(cross_in.at[j], cross_in.at[j], x_send.at[0], x_recv.at[j], beside).wait_recv()
            here = slice(j * cols, (j + 1) * cols)
            both = part[j, :, b].astype(f32) + core_in[j, 0].astype(f32) + cross_in[j].astype(f32)
            out_rows[:, here] = (tokall[b, :, here].astype(f32) + both.reshape(piece, cols)).astype(bf16)

    pl.when(z == 0)(lambda: close(tuple(range(n))))
    pl.when(z > 0)(lambda: close(tuple(range(n - 1, -1, -1))))

    drain(core_in, c_send.at[0])
    drain(cross, x_send.at[0])
    def line_sent(i, carry):
        gone = jnp.logical_or(jnp.logical_and(i <= z, has_up), jnp.logical_and(i > z, has_down))
        pl.when(gone)(lambda: drain(a_shard, w_send.at[2 * i + c]))
        return carry

    lax.fori_loop(0, steps, line_sent, 0)
    drain(upf_ref, y_send.at[0])
    pl.when(has_down)(lambda: drain(a_shard, own_send.at[0]))


def per_device(
    n, tp, tokens, queries, keys, values, lambdas, head_gain, out_weight, mixer_gain, up_weight, down_weight
):
    rows, wide = queries.shape[0], queries.shape[1] // 2
    depth, units = up_weight.shape
    cols = down_weight.shape[1]
    piece, width = tokens.shape
    total = 2 * rows
    vmem = pl.BlockSpec(memory_space=pltpu.VMEM)
    dma = pltpu.SemaphoreType.DMA
    return pl.pallas_call(
        functools.partial(layer_kernel, n, tp),
        out_shape=pltpu.VMEM(tokens.shape, bf16),
        in_specs=[pl.BlockSpec(memory_space=pltpu.SMEM)] + [vmem] * 2 + [pl.BlockSpec(memory_space=pl.ANY)] * 7,
        out_specs=pl.BlockSpec(memory_space=pltpu.VMEM),
        scratch_shapes=[
            pltpu.VMEM(queries.shape, bf16), pltpu.VMEM(keys.shape, bf16), pltpu.VMEM(values.shape, bf16),
            pltpu.VMEM(up_weight.shape, bf16), pltpu.VMEM(down_weight.shape, bf16), pltpu.VMEM(tokens.shape, bf16),
            pltpu.VMEM((tp, piece, 2 * tp * wide), bf16),
            pltpu.VMEM((n * depth, units), bf16),
            pltpu.VMEM((n, units, cols), bf16),
            pltpu.VMEM((2, total, wide), bf16),
            pltpu.VMEM((n // 2, 2, total, wide), bf16),
            pltpu.VMEM((2, 2 * total, wide), bf16),
            pltpu.VMEM((2, 2 * total, 128), f32),
            pltpu.VMEM((2, 2 * total, 128), f32),
            pltpu.VMEM((2, 2 * total, wide), f32),
            pltpu.VMEM((2, tp, 2, piece, wide), bf16),
            pltpu.VMEM(out_weight.shape, bf16),
            pltpu.VMEM((tp, piece, width), bf16),
            pltpu.VMEM((2, 2 * piece, width), bf16),
            pltpu.VMEM((2, 2 * piece, units), bf16),
            pltpu.VMEM((n, 2, tp, piece // 2, cols), bf16),
            pltpu.VMEM((n, 2, 2, piece // 2, cols), bf16),
            pltpu.VMEM((n, 2, piece // 2, cols), bf16),
            pltpu.VMEM((n, 2, piece // 2, cols), bf16),
            dma((3,)), dma((3,)), dma((2,)), dma((1,)), dma((4,)), dma((4,)),
            dma((n // 2,)), dma((n // 2, 2)),
            dma((n,)), dma((1,)), dma((1,)), dma((n, CHUNKS)), dma((2,)), dma((2,)),
            dma((1,)), dma((1,)), dma((7,)), dma((2,)), dma((2,)), dma((6,)),
            dma((1,)), dma((n,)), dma((n, 2)), dma((1,)), dma((n,)),
        ],
        compiler_params=pltpu.CompilerParams(
            collective_id=0, has_side_effects=True, vmem_limit_bytes=60 * 1024 * 1024
        ),
    )(
        lambdas, head_gain.reshape(1, -1), mixer_gain.reshape(1, -1), queries, keys, values, up_weight, down_weight,
        tokens, out_weight,
    )


def solution(mesh):
    placed = (
        P(("sp", "tp"), None),
        P("sp", "tp"),
        P("sp", "tp"),
        P("sp", "tp"),
        P("tp"),
        P(),
        P(),
        P(),
        P("sp", "tp"),
        P("tp", "sp"),
    )
    return jax.shard_map(
        functools.partial(per_device, mesh.shape["sp"], mesh.shape["tp"]),
        mesh=mesh,
        in_specs=placed,
        out_specs=P(("sp", "tp"), None),
        check_vma=False,
    )
```

```python
import functools

import jax
import jax.numpy as jnp
from jax import lax
from jax.experimental import pallas as pl
from jax.experimental.pallas import tpu as pltpu
from jax.sharding import PartitionSpec as P

DQK = 64
MESH = pl.DeviceIdType.MESH
f32, bf16 = jnp.float32, jnp.bfloat16
CHUNKS = 4
UPS, DOWNS = (0, 1), (2, 3)


def layer_kernel(
    n, tp,
    lam_ref, gain_ref, mix_ref, q_hbm, k_hbm, v_hbm, up_hbm, dn_hbm, tok_hbm, ow_hbm,
    out_rows,
    q_ref, k_ref, v_ref, up_ref, dn_ref, tok_ref,
    ah, upf_ref, dnf_ref,
    qb, kv, qm, run_max, run_sum, acc, att, ow, tokall, normed, hid, part, core_in, cross, cross_in,
    ex_send, ex_recv, top_recv, swap_send, tk_send, tk_recv, kv_send, kv_recv,
    w_send, own_send, y_send, w_recv, u_send, u_recv, a_send, a_recv, loc, own_att, in_sem,
    c_send, first_recv, c_recv, x_send,
):
    s = lax.axis_index("sp")
    t = lax.axis_index("tp")
    z, y = s // 2, lax.rem(s, 2)
    x, c = t // 2, lax.rem(t, 2)
    steps = n // 2
    rows = q_ref.shape[0]
    wide = q_ref.shape[1] // 2
    total = 2 * rows
    piece = rows // tp
    top, helper = z == steps - 1, z == steps - 2
    has_up, has_down = z < steps - 1, z > 0
    above, below = (s + 2, t), (s - 2, t)
    beside = (s + 1 - 2 * y, t)
    core = (s, t + 1 - 2 * c)
    across_x = (s, lax.rem(t + 2, tp))
    line = 2 * z + c
    own_line = y == c
    partner = (line, 2 * x + y)

    fetched = []
    for i, (src, dst) in enumerate((
        (k_hbm, k_ref), (v_hbm, v_ref), (q_hbm, q_ref), (up_hbm, up_ref), (dn_hbm, dn_ref), (tok_hbm, tok_ref)
    )):
        fetched.append(pltpu.make_async_copy(src, dst, in_sem.at[i]))
        fetched[-1].start()

    barrier = pltpu.get_barrier_semaphore()

    def greet(device):
        pl.semaphore_signal(barrier, inc=1, device_id=device, device_id_type=MESH)

    for e in range(2):
        for i in range(tp):
            who = (2 * z + e, i)

            @pl.when(jnp.logical_or(e != y, i != t))
            def _():
                greet(who)

    pl.when(has_up)(lambda: greet(above))
    pl.when(has_down)(lambda: greet(below))
    pl.semaphore_wait(barrier, 2 * tp - 1 + has_up.astype(jnp.int32) + has_down.astype(jnp.int32))

    for copy in fetched:
        copy.wait()

    def remote(src, dst, send, recv, device):
        return pltpu.make_async_remote_copy(
            src_ref=src, dst_ref=dst, send_sem=send, recv_sem=recv, device_id=device, device_id_type=MESH
        )

    def drain(ref, sem):
        remote(ref, ref, sem, sem, beside).wait_send()

    def rows_of(e):
        return pl.ds(pl.multiple_of(e * rows, rows), rows)

    def cols_of(e):
        return pl.ds(pl.multiple_of(e * wide, wide), wide)

    my_rows, peer_rows = rows_of(y), rows_of(1 - y)
    my_cols, peer_cols = cols_of(y), cols_of(1 - y)
    qkv = (q_ref, k_ref, v_ref)

    def landing(i, plane, slot, where):
        return qb.at[slot, where] if i == 0 else kv.at[plane, i - 1, where]

    def exchange(i, where):
        return remote(
            qkv[i].at[:, peer_cols], landing(i, z, 0, where), ex_send.at[0], ex_recv.at[i], beside
        )

    def lower(i, e):
        where = my_rows if e == 0 else peer_rows
        src = qkv[i].at[:, my_cols] if e == 0 else landing(i, z, 0, where)
        return remote(src, landing(i, z, 1, where), ex_send.at[1 + e], top_recv.at[y if e == 0 else 1 - y], below)

    def kv_part(j, r, i):
        part_of = kv.at[j, i, rows_of(r)]
        return remote(part_of, part_of, kv_send.at[j], kv_recv.at[j, r], above)

    def own_kv(i):
        return remote(
            qkv[1 + i].at[:, my_cols], kv.at[z, i, my_rows], kv_send.at[z], kv_recv.at[z, y], above
        )

    kv_rises = z < steps - 2
    for i in (1, 2, 0):
        exchange(i, my_rows).start()

    @pl.when(kv_rises)
    def _():
        for i in range(2):
            own_kv(i).start()

    @pl.when(top)
    def _():
        for i in range(3):
            lower(i, 0).start()

    depth, units = up_ref.shape
    half_depth, half = depth // 2, units // 2

    def shard(k, j):
        if k in UPS:
            return upf_ref.at[pl.ds(pl.multiple_of(j * depth + k * half_depth, half_depth), half_depth)]
        return dnf_ref.at[j, slice((k - 2) * half, (k - 1) * half)]

    given = (
        up_ref.at[slice(0, half_depth)], up_ref.at[slice(half_depth, depth)],
        dn_ref.at[slice(0, half)], dn_ref.at[slice(half, units)],
    )

    def swap(k):
        return remote(given[k], shard(k, s), swap_send.at[0], w_recv.at[s, k], partner)

    def send_above(k, j, src):
        remote(src, shard(k, j), w_send.at[j], w_recv.at[j, k], above).start()

    def send_below(k, j, src, sems):
        remote(src, shard(k, j), sems, w_recv.at[j, k], below).start()

    def over(k, j, src):
        remote(src, shard(k, j), y_send.at[0], w_recv.at[j, k], core).start()

    early_down = jnp.logical_or(z == 0, helper)

    def own_above(k, src):
        pl.when(has_up)(lambda: send_above(k, line, src))

    def own_around(k, src):
        pl.when(has_down)(lambda: send_below(k, line, src, own_send.at[0]))
        over(k, line, src)

    @pl.when(own_line)
    def _():
        for k in UPS:
            own_above(k, given[k])
            pl.when(jnp.logical_not(top))(lambda: own_around(k, given[k]))
        for k in DOWNS:
            pl.when(helper)(lambda: own_above(k, given[k]))

    @pl.when(jnp.logical_not(own_line))
    def _():
        for k in UPS + DOWNS:
            swap(k).start()

    b = 2 * y + x
    bx = b + 1 - 2 * x
    by = lax.rem(b + 2, tp)
    bd = lax.rem(bx + 2, tp)

    half_piece = piece // 2

    def token_own(k):
        return remote(tok_ref, tokall.at[b], tk_send.at[k], tk_recv.at[k], (across_x, beside)[k])

    def token_half(k):
        source = (bx, by)[k]
        moved = tokall.at[source, pl.ds(k * half_piece, half_piece)]
        return remote(moved, moved, tk_send.at[2 + k], tk_recv.at[2 + k], (beside, across_x)[k])

    token_own(0).start()

    def local_copy(i):
        src, dst = (
            (k_ref.at[:, my_cols], kv.at[z, 0, my_rows]),
            (v_ref.at[:, my_cols], kv.at[z, 1, my_rows]),
            (q_ref.at[:, my_cols], qb.at[0, my_rows]),
            (up_ref, upf_ref.at[pl.ds(pl.multiple_of(s * depth, depth), depth)]),
            (dn_ref, dnf_ref.at[s]),
            (ow_hbm, ow),
            (tok_ref, tokall.at[b]),
        )[i]
        return pltpu.make_async_copy(src, dst, loc.at[i])

    for i in range(3):
        local_copy(i).start()

    @pl.when(own_line)
    def _():
        local_copy(3).start()
        local_copy(4).start()

    local_copy(5).start()
    local_copy(6).start()

    for i in range(3):
        local_copy(i).wait()
    for i in (1, 2, 0):
        exchange(i, peer_rows).wait_recv()
        if i > 0:
            pl.when(kv_rises)(lambda: kv_part(z, 1 - y, i - 1).start())

    @pl.when(top)
    def _():
        for i in range(3):
            lower(i, 1).start()

    @pl.when(own_line)
    def _():
        for k in UPS:
            pl.when(top)(lambda: own_around(k, given[k]))
        for k in DOWNS:
            pl.when(z == 0)(lambda: own_above(k, given[k]))
            own_around(k, given[k])

    def await_chunk(k, j):
        moved = shard(k, j)
        remote(moved, moved, w_send.at[j], w_recv.at[j, k], core).wait_recv()

    def from_core(k, i):
        await_chunk(k, 2 * i + 1 - c)

    def swapped(ks):
        @pl.when(jnp.logical_not(own_line))
        def _():
            for k in ks:
                await_chunk(k, line)
                src = shard(k, line)
                if k in UPS:
                    own_above(k, src)
                else:
                    pl.when(early_down)(lambda: own_above(k, src))
                own_around(k, src)

    def late_down():
        @pl.when(own_line)
        def _():
            for k in DOWNS:
                own_above(k, given[k])

        @pl.when(jnp.logical_not(own_line))
        def _():
            for k in DOWNS:
                own_above(k, shard(k, line))

    def from_above(d, ks):
        j = line + 2 * d
        for k in ks:
            await_chunk(k, j)
            src = shard(k, j)
            pl.when(has_down)(lambda: send_below(k, j, src, w_send.at[j]))
            over(k, j, src)

    def from_below(d, ks):
        j = line - 2 * d
        for k in ks:
            await_chunk(k, j)
            src = shard(k, j)
            pl.when(has_up)(lambda: send_above(k, j, src))
            over(k, j, src)

    chunk = rows
    lane = lax.broadcasted_iota(jnp.int32, (total, wide), 1)

    def weigh(sc, top_row):
        parts, whole = [], None
        for i in range(sc.shape[1] // 128):
            p = jnp.exp(sc[:, i * 128:(i + 1) * 128] - top_row)
            whole = p if whole is None else whole + p
            parts.append(p.astype(bf16))
        return jnp.concatenate(parts, axis=1), whole

    def scores_of(u, r0, j, keys):
        return lax.dot_general(
            qm[u, pl.ds(r0, chunk), :], kv[j, 0, :keys, :], (((1,), (1,)), ((), ())), preferred_element_type=f32
        )

    def diagonal(u, carry):
        @pl.when(u == 1)
        def _():
            for e in range(2):
                three = qm.at[1, slice(0, 3 * rows)]
                remote(three, three, ex_send.at[0], top_recv.at[e], above).wait_recv()

        scaled = qb[u] * jnp.asarray(DQK ** -0.5, bf16)
        for m in range(2):
            qm[u, m * total:(m + 1) * total, :] = jnp.where((lane < DQK) == (m == 0), scaled, jnp.zeros_like(scaled))
        j = z + u
        for m in range(2):
            for i in range(total // chunk):
                r0, keys = m * total + i * chunk, (i + 1) * chunk
                here = pl.ds(r0, chunk)
                sc = scores_of(u, r0, j, keys)
                qpos = i * chunk + lax.broadcasted_iota(jnp.int32, (chunk, keys), 0)
                kpos = lax.broadcasted_iota(jnp.int32, (chunk, keys), 1)
                sc = jnp.where(kpos <= qpos, sc, -jnp.inf)
                top_row = jnp.broadcast_to(jnp.max(sc, axis=1, keepdims=True), (chunk, 128))
                p, whole = weigh(sc, top_row)
                run_max[u, here, :] = top_row
                run_sum[u, here, :] = whole
                acc[u, here, :] = jnp.dot(p, kv[j, 1, :keys, :], preferred_element_type=f32)
        return carry

    def tile(u, j, r0):
        here = pl.ds(r0, chunk)
        sc = scores_of(u, r0, j, total)
        old = run_max[u, here, :]
        top_row = jnp.maximum(old, jnp.max(sc, axis=1, keepdims=True))
        p, whole = weigh(sc, top_row)
        shrink = jnp.exp(old - top_row)
        run_max[u, here, :] = top_row
        run_sum[u, here, :] = run_sum[u, here, :] * shrink + whole
        acc[u, here, :] = acc[u, here, :] * shrink + jnp.dot(p, kv[j, 1], preferred_element_type=f32)

    def tiles(u, j, hh):
        def one(m, carry):
            tile(u, j, pl.multiple_of(m * total + hh * rows, rows))
            return carry

        lax.fori_loop(0, 2, one, 0)

    def finish(u, hh):
        lam = lam_ref[y]
        maps = []
        for m in range(2):
            here = pl.ds(pl.multiple_of(m * total + hh * rows, rows), rows)
            maps.append(acc[u, here, :] / jnp.sum(run_sum[u, here, :], axis=1, keepdims=True))
        differ = maps[0] - lam * maps[1]
        spread_of = lax.rsqrt(jnp.mean(differ * differ, axis=1, keepdims=True) + 1e-06)
        done = (differ * spread_of * gain_ref[...]).astype(bf16)
        att[u, pl.ds(hh * (tp // 2), tp // 2)] = done.reshape(tp // 2, 2, piece, wide)

    def side(hh):
        return pl.ds(hh * (tp // 2), tp // 2)

    def raise_att(hh):
        return remote(att.at[1, side(hh)], att.at[0, side(hh)], u_send.at[hh], u_recv.at[hh], above)

    head = 2 * t + y

    def head_cols(i):
        return pl.ds(pl.multiple_of(i * wide, wide), wide)

    def to_tokens(hh, e, i, owner):
        return remote(
            att.at[0, side(hh), i % 2], ah.at[side(hh), :, head_cols(owner)],
            a_send.at[0], a_recv.at[0], (2 * z + e, i),
        )

    def mine(hh):
        return pltpu.make_async_copy(
            att.at[0, side(hh), c], ah.at[side(hh), :, head_cols(head)], own_att.at[hh]
        )

    def hand_out(hh):
        mine(hh).start()
        for e in range(2):
            for i in range(tp):
                pl.when(jnp.logical_or(e != y, i != t))(lambda: to_tokens(hh, e, i, head).start())

    def spread():
        swapped(DOWNS)

        @pl.when(own_line)
        def _():
            for k in DOWNS:
                from_core(k, z)

        token_own(1).start()

    def pass_tokens():
        for k in (1, 0):
            token_own(k).wait_recv()
            token_half(k).start()

    @pl.when(jnp.logical_not(top))
    def _():
        diagonal(0, 0)

    swapped(UPS)
    forwarded = jnp.logical_and(helper, own_line)
    pl.when(forwarded)(lambda: from_below(1, UPS))

    @pl.when(helper)
    def _():
        spread()
        lax.fori_loop(1, 2, diagonal, 0)
        for hh in range(2):
            tiles(1, z, hh)

    middle = jnp.logical_and(z > 0, kv_rises)
    pl.when(jnp.logical_or(z == 0, top))(spread)

    def block(d, carry):
        j = z - d
        for r in (y, 1 - y):
            moved = kv.at[j, :, rows_of(r)]
            remote(moved, moved, kv_send.at[j], kv_recv.at[j, r], above).wait_recv()
            for i in range(2):
                pl.when(kv_rises)(lambda: kv_part(j, r, i).start())

        forward_now = jnp.logical_and(d == jnp.where(helper, 1, 2), jnp.logical_not(forwarded))
        pl.when(forward_now)(lambda: from_below(1, UPS))
        pl.when(jnp.logical_and(helper, d == 2))(pass_tokens)

        def ahead():
            from_above(1, DOWNS[1:])
            from_below(2, UPS[:1])

        def slot(v, inner):
            u, hh = 1 - v // 2, lax.rem(v, 2)
            own_turn = jnp.logical_and(v == 2, helper)
            pl.when(jnp.logical_and(own_turn, d == 1))(lambda: from_above(1, UPS))
            pl.when(jnp.logical_and(own_turn, d == 2))(lambda: from_above(1, DOWNS[:1]))
            pl.when(jnp.logical_and(helper, jnp.logical_and(v == 3, d == 2)))(ahead)
            tiles(u, j, hh)

            @pl.when(d == z)
            def _():
                finish(u, hh)
                pl.when(u == 1)(lambda: raise_att(hh).start())
                pl.when(u == 0)(lambda: hand_out(hh))

            return inner

        lax.fori_loop(jnp.where(helper, 0, 2), 4, slot, 0)
        pl.when(jnp.logical_and(d == 1, middle))(spread)
        pl.when(jnp.logical_and(d == 1, kv_rises))(lambda: from_above(1, UPS))
        pl.when(jnp.logical_and(d == 2, kv_rises))(lambda: from_above(1, DOWNS))
        return carry

    lax.fori_loop(1, jnp.where(top, 1, z + 1), block, 0)

    @pl.when(z == 0)
    def _():
        for hh in range(2):
            finish(0, hh)
            hand_out(hh)

    @pl.when(top)
    def _():
        from_below(1, UPS)
        pass_tokens()
        from_below(1, DOWNS)
        from_below(2, UPS)
        for hh in range(2):
            raise_att(hh).wait_recv()
            hand_out(hh)

    @pl.when(z == 0)
    def _():
        from_above(1, UPS + DOWNS)
        pass_tokens()

    @pl.when(z == 1)
    def _():
        pl.when(jnp.logical_not(forwarded))(lambda: from_below(1, UPS))
        late_down()
        from_above(1, DOWNS[:1])
        from_above(2, UPS)
        from_above(1, DOWNS[1:])
        from_below(1, DOWNS)
        pass_tokens()
        from_above(2, DOWNS)

    @pl.when(jnp.logical_and(z >= 2, has_up))
    def _():
        pl.when(jnp.logical_not(helper))(pass_tokens)
        pl.when(jnp.logical_not(helper))(lambda: from_below(2, UPS[:1]))
        from_below(2, UPS[1:])
        pl.when(helper)(lambda: from_below(1, DOWNS[:1]))

    @pl.when(top)
    def _():
        from_below(3, UPS)

    local_copy(5).wait()
    local_copy(6).wait()
    for hh in range(2):
        mine(hh).wait()
    for k in range(2):
        token_half(k).wait_recv()
        token_half(k).wait_send()
    others = ah.at[:, :, slice(0, (2 * tp - 1) * wide)]
    remote(others, others, a_send.at[0], a_recv.at[0], beside).wait_recv()

    def project(hf):
        part_rows = slice(hf * half_piece, (hf + 1) * half_piece)
        heads = ah[:, part_rows, :].reshape(2 * piece, 2 * tp * wide)
        projected = jnp.dot(heads, ow[...], preferred_element_type=f32).astype(bf16)
        given_tokens = tokall[:, part_rows, :].reshape(projected.shape).astype(f32)
        summed = (given_tokens + projected.astype(f32)).astype(bf16)
        tokall[:, part_rows, :] = summed.reshape(tp, half_piece, summed.shape[1])
        summed = summed.astype(f32)
        scale = lax.rsqrt(jnp.mean(summed * summed, axis=1, keepdims=True) + 1e-06)
        normed[hf] = (summed * scale * mix_ref[...]).astype(bf16)

    project(0)
    pl.when(helper)(lambda: from_below(1, DOWNS[1:]))

    def later_ups(d, carry):
        pl.when(jnp.logical_and(z + d < steps, jnp.logical_or(z != 1, d != 2)))(lambda: from_above(d, UPS))
        waits = jnp.logical_and(d >= 3, jnp.logical_not(jnp.logical_and(top, d == 3)))
        pl.when(jnp.logical_and(z - d >= 0, waits))(lambda: from_below(d, UPS))
        return carry

    lax.fori_loop(2, steps, later_ups, 0)
    pl.when(jnp.logical_and(z > 1, kv_rises))(late_down)
    pl.when(jnp.logical_and(z > 1, kv_rises))(lambda: from_below(1, DOWNS))

    @pl.when(own_line)
    def _():
        local_copy(3).wait()
        local_copy(4).wait()

    def order(k):
        return jnp.where(k < steps - z, z + k, steps - 1 - k)

    def up_pair(k, carry):
        for m in UPS:
            from_core(m, k)
        return carry

    lax.fori_loop(0, steps, up_pair, 0)

    def unit(hf):
        inner = jnp.dot(normed[hf], upf_ref[...], preferred_element_type=f32)
        hid[hf] = jnp.square(jnp.maximum(inner, 0.0)).astype(bf16)

    first = ((across_x, bx), (beside, by))

    def to_first(j, e, m, hf):
        device, where = first[e]
        return remote(
            part.at[j, hf, where if m == 0 else bd], core_in.at[j, m, hf],
            c_send.at[0], (first_recv.at[j] if m == 0 else c_recv.at[j, hf]), device,
        )

    def to_second(j, e, hf):
        return remote(
            cross.at[j, hf], cross_in.at[j, hf], x_send.at[0], first_recv.at[j], first[1 - e][0]
        )

    def relay(i, hf):
        for e in range(2):
            j = 2 * i + e
            to_first(j, e, 1, hf).wait_recv()
            where = first[1 - e][1]
            cross[j, hf] = (part[j, hf, where].astype(f32) + core_in[j, 1, hf].astype(f32)).astype(bf16)
            to_second(j, e, hf).start()

    def multiply(i, hfs):
        for hf in hfs:
            for e in range(2):
                j = 2 * i + e
                product = jnp.dot(hid[hf], dnf_ref[j], preferred_element_type=f32).astype(bf16)
                part[j, hf] = product.reshape(tp, half_piece, product.shape[1])
            for e in range(2):
                to_first(2 * i + e, e, 1, hf).start()
        for hf in hfs:
            for e in range(2):
                to_first(2 * i + e, e, 0, hf).start()

    def arrivals(k):
        i = order(k)
        pl.when(i - z >= jnp.where(z == 1, 3, 2))(lambda: from_above(i - z, DOWNS))
        pl.when(z - i >= jnp.where(helper, 3, 2))(lambda: from_below(z - i, DOWNS))
        for m in DOWNS:
            pl.when(jnp.logical_not(jnp.logical_and(own_line, i == z)))(lambda: from_core(m, i))

    ready = 2
    unit(0)

    def early_pair(k, carry):
        arrivals(k)
        multiply(order(k), (0,))
        return carry

    lax.fori_loop(0, ready, early_pair, 0)
    project(1)
    unit(1)
    pl.when(helper)(lambda: from_below(2, DOWNS[:1]))

    def second_pair(k, carry):
        relay(order(k), 0)
        multiply(order(k), (1,))
        return carry

    lax.fori_loop(0, ready, second_pair, 0)
    pl.when(helper)(lambda: from_below(2, DOWNS[1:]))
    edge = jnp.logical_or(top, z == 0)

    def relay_both(k):
        for hf in range(2):
            relay(order(k), hf)

    def late_pair(k, carry):
        final = k == steps - 1
        pl.when(jnp.logical_and(edge, final))(lambda: relay_both(k - 1))
        arrivals(k)
        multiply(order(k), (0, 1))

        @pl.when(k == ready)
        def _():
            for i in range(ready):
                relay(order(i), 1)

        pl.when(jnp.logical_and(k > ready, jnp.logical_not(jnp.logical_and(edge, final))))(lambda: relay_both(k - 1))
        return carry

    lax.fori_loop(ready, steps, late_pair, 0)
    for k in range(2):
        token_own(k).wait_send()
    drain(others, a_send.at[0])
    three = qm.at[0, slice(0, 3 * rows)]
    drain(three, ex_send.at[0])

    @pl.when(top)
    def _():
        for e in range(2):
            drain(three, ex_send.at[1 + e])

    a_shard = upf_ref.at[slice(0, 2 * depth)]
    pl.when(jnp.logical_not(own_line))(lambda: drain(a_shard, swap_send.at[0]))

    @pl.when(helper)
    def _():
        for hh in range(2):
            raise_att(hh).wait_send()

    @pl.when(kv_rises)
    def _():
        def sent(j, carry):
            drain(kv.at[j], kv_send.at[j])
            return carry

        lax.fori_loop(0, z + 1, sent, 0)

    relay_both(steps - 1)
    cols = dn_ref.shape[1]
    def close(js):
        for at, j in enumerate(js):
            both_in = core_in.at[j]
            remote(both_in, both_in, c_send.at[0], first_recv.at[j], beside).wait_recv()
            here = slice(j * cols, (j + 1) * cols)
            both = part[j, :, b].astype(f32) + core_in[j, 0].astype(f32) + cross_in[j].astype(f32)
            out_rows[:, here] = (tokall[b, :, here].astype(f32) + both.reshape(piece, cols)).astype(bf16)

    pl.when(z == 0)(lambda: close(tuple(range(n))))
    pl.when(z > 0)(lambda: close(tuple(range(n - 1, -1, -1))))

    drain(core_in, c_send.at[0])
    drain(cross, x_send.at[0])
    def line_sent(i, carry):
        gone = jnp.logical_or(jnp.logical_and(i <= z, has_up), jnp.logical_and(i > z, has_down))
        pl.when(gone)(lambda: drain(a_shard, w_send.at[2 * i + c]))
        return carry

    lax.fori_loop(0, steps, line_sent, 0)
    drain(upf_ref, y_send.at[0])
    pl.when(has_down)(lambda: drain(a_shard, own_send.at[0]))


def per_device(
    n, tp, tokens, queries, keys, values, lambdas, head_gain, out_weight, mixer_gain, up_weight, down_weight
):
    rows, wide = queries.shape[0], queries.shape[1] // 2
    depth, units = up_weight.shape
    cols = down_weight.shape[1]
    piece, width = tokens.shape
    total = 2 * rows
    vmem = pl.BlockSpec(memory_space=pltpu.VMEM)
    dma = pltpu.SemaphoreType.DMA
    return pl.pallas_call(
        functools.partial(layer_kernel, n, tp),
        out_shape=pltpu.VMEM(tokens.shape, bf16),
        in_specs=[pl.BlockSpec(memory_space=pltpu.SMEM)] + [vmem] * 2 + [pl.BlockSpec(memory_space=pl.ANY)] * 7,
        out_specs=pl.BlockSpec(memory_space=pltpu.VMEM),
        scratch_shapes=[
            pltpu.VMEM(queries.shape, bf16), pltpu.VMEM(keys.shape, bf16), pltpu.VMEM(values.shape, bf16),
            pltpu.VMEM(up_weight.shape, bf16), pltpu.VMEM(down_weight.shape, bf16), pltpu.VMEM(tokens.shape, bf16),
            pltpu.VMEM((tp, piece, 2 * tp * wide), bf16),
            pltpu.VMEM((n * depth, units), bf16),
            pltpu.VMEM((n, units, cols), bf16),
            pltpu.VMEM((2, total, wide), bf16),
            pltpu.VMEM((n // 2, 2, total, wide), bf16),
            pltpu.VMEM((2, 2 * total, wide), bf16),
            pltpu.VMEM((2, 2 * total, 128), f32),
            pltpu.VMEM((2, 2 * total, 128), f32),
            pltpu.VMEM((2, 2 * total, wide), f32),
            pltpu.VMEM((2, tp, 2, piece, wide), bf16),
            pltpu.VMEM(out_weight.shape, bf16),
            pltpu.VMEM((tp, piece, width), bf16),
            pltpu.VMEM((2, 2 * piece, width), bf16),
            pltpu.VMEM((2, 2 * piece, units), bf16),
            pltpu.VMEM((n, 2, tp, piece // 2, cols), bf16),
            pltpu.VMEM((n, 2, 2, piece // 2, cols), bf16),
            pltpu.VMEM((n, 2, piece // 2, cols), bf16),
            pltpu.VMEM((n, 2, piece // 2, cols), bf16),
            dma((3,)), dma((3,)), dma((2,)), dma((1,)), dma((4,)), dma((4,)),
            dma((n // 2,)), dma((n // 2, 2)),
            dma((n,)), dma((1,)), dma((1,)), dma((n, CHUNKS)), dma((2,)), dma((2,)),
            dma((1,)), dma((1,)), dma((7,)), dma((2,)), dma((6,)),
            dma((1,)), dma((n,)), dma((n, 2)), dma((1,)),
        ],
        compiler_params=pltpu.CompilerParams(
            collective_id=0, has_side_effects=True, vmem_limit_bytes=60 * 1024 * 1024
        ),
    )(
        lambdas, head_gain.reshape(1, -1), mixer_gain.reshape(1, -1), queries, keys, values, up_weight, down_weight,
        tokens, out_weight,
    )


def solution(mesh):
    placed = (
        P(("sp", "tp"), None),
        P("sp", "tp"),
        P("sp", "tp"),
        P("sp", "tp"),
        P("tp"),
        P(),
        P(),
        P(),
        P("sp", "tp"),
        P("tp", "sp"),
    )
    return jax.shard_map(
        functools.partial(per_device, mesh.shape["sp"], mesh.shape["tp"]),
        mesh=mesh,
        in_specs=placed,
        out_specs=P(("sp", "tp"), None),
        check_vma=False,
    )
```
